512 devices in a mesh: sp: 32 (over z, x), tp: 16 (over y, core).
Axes of the slice: x: 4, y: 8, z: 8, core: 2. Of those that a mesh axis runs over, the one named last changes fastest.
Arguments:
- queries: bfloat16 [8192, 2048], P('sp', 'tp'), may hold values from -6 to 6
- key_matrix: bfloat16 [8192, 2048], P('sp', 'tp'), may hold values from -6 to 6
- value_matrix: bfloat16 [8192, 4096], P('sp', 'tp'), may hold values from -6 to 6
- output_gate_preactivation: bfloat16 [8192, 4096], P('sp', 'tp'), may hold values from -6 to 6
- decay_preactivation: bfloat16 [8192, 2048], P('sp', 'tp')
- extra_log_decay: float32 [8192, 16], P('sp', 'tp'), may hold values from -0.7 to 0
- head_norm_gain: bfloat16 [256], replicated, may hold values from 0.099609375 to 1.8984375
- output_projection: bfloat16 [4096, 2048], P(None, 'tp'), may hold values from -0.09375 to 0.09375
- residual: bfloat16 [8192, 2048], P('sp', 'tp'), may hold values from -210 to 210
- feedforward_gain: bfloat16 [2048], replicated, may hold values from 0.099609375 to 1.8984375
- routing: int32 [8192, 4], P('sp'), may hold values from 0 to 127, all different within a row; in each aligned block of 256 rows (0 to 255, 256 to 511, ...) at most 12 rows name the same one
- router_score: float32 [8192, 4], P('sp'), may hold values from 0.05 to 1
- expert_gate_weight: bfloat16 [2048, 131072], P(None, ('sp', 'tp')), may hold values from -0.125 to 0.125
- expert_up_weight: bfloat16 [2048, 131072], P(None, ('sp', 'tp')), may hold values from -0.125 to 0.125
- expert_down_weight: bfloat16 [131072, 2048], P(('sp', 'tp')), may hold values from -0.1875 to 0.1875
- shared_expert_gate: bfloat16 [2048, 512], P(None, 'tp'), may hold values from -0.125 to 0.125
- shared_expert_up: bfloat16 [2048, 512], P(None, 'tp'), may hold values from -0.125 to 0.125
- shared_expert_down: bfloat16 [512, 2048], P(None, 'tp'), may hold values from -0.25 to 0.25
Outputs:
- layer_out: bfloat16 [8192, 2048], P('sp', 'tp')
The draws below stay inside these ranges and needn't reach their ends.
Inputs may be any that keep to these rules, and one draw needn't show every extreme that they name: `routing`: each row names 4 different experts. In each aligned block of 256 rows, the rows of one index of sp, no expert is named by more than 12 rows, a bound that some expert reaches in some blocks.
All inputs are finite; a program needn't handle non-finite values.
Results may differ from the reference program's by a relative error of at most 0.01.
Values may be sent and summed in bfloat16 or wider, within the bound.
No kernel may reach another device: no remote copies, remote signals or barrier semaphores. Data moves between devices by JAX's collectives and lax.ppermute only.
A program may use at most 64 MiB of HBM per device.

```python
import math
import jax
import jax.numpy as jnp
import numpy as np
from jax import lax

D = 2048
ATTENTION_HEADS = 16
DK = 128
DV = 256
BLOCK_POSITIONS = 64
FF = 1024
SF = 512
K = 4
TOK_DEV = 256
SEQUENCE_LENGTH = 8192
E = 128
MOST = 12
N_SP = 32


def draw_decay_preactivation(key, part):
    key_head, key_block, key_jitter = jax.random.split(key, 3)
    head_kind = jax.random.randint(key_head, (ATTENTION_HEADS,), 0, 2)
    slow_head = head_kind.astype(jnp.float32)
    slow_level = math.log(SEQUENCE_LENGTH / 4.0)
    base_level = 0.7 + slow_head * (slow_level - 0.7)
    block_shift = jax.random.uniform(key_block, (SEQUENCE_LENGTH // BLOCK_POSITIONS, 1, 1, 1), jnp.float32, -0.7, 0.7)
    jitter = jnp.clip(jax.random.normal(key_jitter, (SEQUENCE_LENGTH // BLOCK_POSITIONS, BLOCK_POSITIONS, ATTENTION_HEADS, DK), jnp.float32), -2.5, 2.5)
    logit = base_level[None, None, :, None] + block_shift + jitter
    return logit.reshape(SEQUENCE_LENGTH, ATTENTION_HEADS * DK).astype(jnp.bfloat16)


def draw_extra_log_decay(key, part):
    key_place, key_width = jax.random.split(key)
    third = SEQUENCE_LENGTH // 3
    position_list = jnp.arange(3, dtype=jnp.int32)[:, None] * third + jax.random.randint(key_place, (3, ATTENTION_HEADS), 0, third)
    spike_magnitude = jnp.log(jax.random.uniform(key_width, (3, ATTENTION_HEADS), jnp.float32, 0.5, 0.8))
    spike_positions = (jnp.arange(SEQUENCE_LENGTH, dtype=jnp.int32)[:, None, None] == position_list[None]).astype(jnp.float32)
    return jnp.sum(spike_positions * spike_magnitude[None], axis=1)


def draw_residual(key, part):
    key_row, key_col, key_value = jax.random.split(key, 3)
    column_pos = jnp.arange(D, dtype=jnp.float32) / D
    row_scale = jnp.exp(jax.random.uniform(key_row, (SEQUENCE_LENGTH,), jnp.float32, math.log(0.3), math.log(3.0)))
    column_rise = math.log(5.0)
    column_scale = 0.5 * jnp.exp(column_rise * column_pos) * jax.random.uniform(key_col, (D,), jnp.float32, 0.7, 1.4)
    values = jnp.clip(jax.random.normal(key_value, (SEQUENCE_LENGTH, D), jnp.float32), -5.0, 5.0)
    return (values * row_scale[:, None] * column_scale[None, :]).astype(jnp.bfloat16)


def level_of(own_key, shape, cuts, least, top_value):
    loudness, own = 1.0, jax.random.fold_in(own_key, 6)
    for axis_at, blocks in cuts:
        draws = jnp.exp(jax.random.uniform(jax.random.fold_in(own, axis_at), (blocks,), jnp.float32, least / len(cuts), top_value / len(cuts)))
        loudness = loudness * jnp.repeat(draws, shape[axis_at] // blocks).reshape([-1 if axis == axis_at else 1 for axis in range(len(shape))])
    return loudness


def assign_block(key, own, number, rows, amount, top, bound, slope):
    sequence = jax.random.permutation(key, amount)
    crowded, ordinary = portions_of(amount, rows * top, bound, slope, True), portions_of(amount, rows * top, bound, slope, False)
    places = jnp.arange(amount)

    def named(tallies, offset_by):
        used = int((tallies > 0).sum())
        fixed = max(1, used // 4)
        shifted = fixed + (places - fixed + offset_by * (used - fixed)) % max(1, amount - fixed)
        return jnp.zeros((amount,), jnp.int32).at[sequence[jnp.where(places < fixed, places, shifted)]].set(jnp.asarray(tallies, jnp.int32))

    tallies = jnp.where(number % 4 == 0, named(crowded, number // 4), named(ordinary, number - number // 4 - 1))
    mixed = jax.random.permutation(jax.random.fold_in(own, 3), amount)
    giver, sink = mixed[0:amount // 2 * 2:2], mixed[1:amount // 2 * 2:2]
    slack = jnp.minimum(tallies[giver] - 1, bound - tallies[sink]) // 2
    slack = jnp.where((giver == sequence[0]) | (sink == sequence[0]) | (tallies[sink] == 0), 0, jnp.maximum(slack, 0))
    shifted = jax.random.randint(jax.random.fold_in(own, 4), (amount // 2,), 0, 1 << 20) % (slack + 1)
    tallies = tallies.at[giver].add(-shifted).at[sink].add(shifted)
    labels = jnp.searchsorted(jnp.cumsum(tallies), jnp.arange(rows * top), side="right").astype(jnp.int32)
    grid = labels.reshape(top, rows).T
    grid = grid[jax.random.permutation(jax.random.fold_in(own, 1), rows)]
    offset_by = jax.random.randint(jax.random.fold_in(own, 2), (rows, 1), 0, top)
    return jnp.take_along_axis(grid, (jnp.arange(top)[None, :] + offset_by) % top, axis=1)


def portions_of(count, total, reach, skew, full):
    weights = [(1 << 20) // math.isqrt(grade ** skew) + 1 for grade in range(1, count + 1)]
    largest = reach if full else min(reach, max(-(-total // count), total * weights[0] // sum(weights)))
    least = 1 if total - largest >= count - 1 else 0
    counts, surplus = [largest] + [least] * (count - 1), total - largest - least * (count - 1)
    while surplus > 0:
        candidates = [i for i in range(1, count) if counts[i] < largest] or [i for i in range(1, count) if counts[i] < reach]
        pool, budget = sum([weights[i] for i in candidates]), surplus
        for i in candidates:
            extra = min(reach - counts[i], max(1, budget * weights[i] // pool), surplus)
            counts[i] = counts[i] + extra
            surplus = surplus - extra
    return np.array(counts)


def gaussian(rng, extent, deviation, bound, shards=(), held_as=jnp.bfloat16):
    entries = deviation * jax.random.normal(rng, extent, jnp.float32)
    if shards:
        entries = entries * level_of(rng, extent, shards, -0.22, 0.18)
    return jnp.clip(entries, -bound, bound).astype(held_as)


def setup_inputs(seed: int = 0) -> dict:
    keys = jax.random.split(jax.random.key(seed), 19)
    queries = gaussian(keys[0], (SEQUENCE_LENGTH, ATTENTION_HEADS * DK), 1.0, 6.0, ((0, 32), (1, 16)))
    key_matrix = gaussian(keys[1], (SEQUENCE_LENGTH, ATTENTION_HEADS * DK), 1.0, 6.0, ((0, 32), (1, 16)))
    value_matrix = gaussian(keys[2], (SEQUENCE_LENGTH, ATTENTION_HEADS * DV), 1.0, 6.0, ((0, 32), (1, 16)))
    output_gate_preactivation = gaussian(keys[3], (SEQUENCE_LENGTH, ATTENTION_HEADS * DV), 1.0, 6.0, ((0, 32), (1, 16)))
    decay_preactivation = draw_decay_preactivation(jax.random.fold_in(keys[18], 71), 0)
    extra_log_decay = draw_extra_log_decay(jax.random.fold_in(keys[18], 71), 0)
    head_norm_gain = jnp.clip(1.0 + 0.18 * jax.random.normal(keys[6], (DV,), jnp.float32), 0.099609375, 1.8984375).astype(jnp.bfloat16)
    output_projection = gaussian(keys[7], (ATTENTION_HEADS * DV, D), (ATTENTION_HEADS * DV) ** -0.5, 0.09375, ((1, 16),))
    residual = draw_residual(jax.random.fold_in(keys[18], 71), 0)
    feedforward_gain = jnp.clip(1.0 + 0.18 * jax.random.normal(keys[9], (D,), jnp.float32), 0.099609375, 1.8984375).astype(jnp.bfloat16)
    routing_keys = jax.random.split(jax.random.fold_in(keys[10], 1), SEQUENCE_LENGTH // TOK_DEV)
    routing_turns = jax.random.permutation(jax.random.fold_in(keys[10], 3), SEQUENCE_LENGTH // TOK_DEV)
    routing = jax.vmap(lambda own, number: assign_block(jax.random.fold_in(keys[10], 2), own, number, TOK_DEV, E, K, MOST, 1))(routing_keys, routing_turns).reshape((SEQUENCE_LENGTH, K))
    router_score = jnp.clip(jnp.exp(math.log(1.0) - 2.9957323 * jax.random.uniform(keys[11], (SEQUENCE_LENGTH, K), jnp.float32) ** level_of(keys[11], (SEQUENCE_LENGTH, K), ((0, 32),), -0.2, 0.2)), 0.05, 1.0)
    expert_gate_weight = gaussian(keys[12], (D, E * FF), D ** -0.5, 0.125, ((1, 512),))
    expert_up_weight = gaussian(keys[13], (D, E * FF), D ** -0.5, 0.125, ((1, 512),))
    expert_down_weight = gaussian(keys[14], (E * FF, D), FF ** -0.5, 0.1875, ((0, 512),))
    shared_expert_gate = gaussian(keys[15], (D, SF), D ** -0.5, 0.125, ((1, 16),))
    shared_expert_up = gaussian(keys[16], (D, SF), D ** -0.5, 0.125, ((1, 16),))
    shared_expert_down = gaussian(keys[17], (SF, D), SF ** -0.5, 0.25, ((1, 16),))
    return dict(queries=queries, key_matrix=key_matrix, value_matrix=value_matrix, output_gate_preactivation=output_gate_preactivation, decay_preactivation=decay_preactivation, extra_log_decay=extra_log_decay, head_norm_gain=head_norm_gain, output_projection=output_projection, residual=residual, feedforward_gain=feedforward_gain, routing=routing, router_score=router_score, expert_gate_weight=expert_gate_weight, expert_up_weight=expert_up_weight, expert_down_weight=expert_down_weight, shared_expert_gate=shared_expert_gate, shared_expert_up=shared_expert_up, shared_expert_down=shared_expert_down)


HIGHEST = lax.Precision.HIGHEST
EPSILON = 1e-06
ROUTE_SCALE = 2.5
GATE_TEMPER = 16.0

def attention_check(queries, key_matrix, value_matrix, decay_preactivation, extra_log_decay):
    block_count = SEQUENCE_LENGTH // BLOCK_POSITIONS
    query_block = queries.astype(jnp.float32).reshape(block_count, BLOCK_POSITIONS, ATTENTION_HEADS, DK) * DK ** (-0.5)
    key_block = key_matrix.astype(jnp.float32).reshape(block_count, BLOCK_POSITIONS, ATTENTION_HEADS, DK)
    value_block = value_matrix.astype(jnp.float32).reshape(block_count, BLOCK_POSITIONS, ATTENTION_HEADS, DV)
    log_decay_rows = jax.nn.log_sigmoid(decay_preactivation.astype(jnp.float32)).reshape(block_count, BLOCK_POSITIONS, ATTENTION_HEADS, DK) / GATE_TEMPER
    log_decay_rows = log_decay_rows + extra_log_decay.reshape(block_count, BLOCK_POSITIONS, ATTENTION_HEADS)[..., None]
    inside = jnp.cumsum(log_decay_rows, axis=1)
    block_total = inside[:, -1]
    query_decay = query_block * jnp.exp(inside)
    key_decay = key_block * jnp.exp(-inside)
    causal = jnp.tril(jnp.ones((BLOCK_POSITIONS, BLOCK_POSITIONS), dtype=bool))
    scores = jnp.where(causal, jnp.einsum('nthd,nshd->nhts', query_decay, key_decay, precision=HIGHEST), 0.0)
    within = jnp.einsum('nhts,nshv->nthv', scores, value_block, precision=HIGHEST)
    key_end = key_block * jnp.exp(block_total[:, None] - inside)

    def advance(carried, inputs):
        decay_sum, keys_end, values, queries_dec = inputs
        readout = jnp.einsum('thd,hdv->thv', queries_dec, carried, precision=HIGHEST)
        fresh_term = jnp.einsum('shd,shv->hdv', keys_end, values, precision=HIGHEST)
        return (jnp.exp(decay_sum)[..., None] * carried + fresh_term, readout)
    start_state = jnp.zeros((ATTENTION_HEADS, DK, DV), jnp.float32)
    _, passed = lax.scan(advance, start_state, (block_total, key_end, value_block, query_decay))
    return (within + passed).reshape(SEQUENCE_LENGTH, ATTENTION_HEADS, DV)

def reference(queries, key_matrix, value_matrix, output_gate_preactivation, decay_preactivation, extra_log_decay, head_norm_gain, output_projection, residual, feedforward_gain, routing, router_score, expert_gate_weight, expert_up_weight, expert_down_weight, shared_expert_gate, shared_expert_up, shared_expert_down):
    attention_output = attention_check(queries, key_matrix, value_matrix, decay_preactivation, extra_log_decay)
    inverse_rms = lax.rsqrt(lax.optimization_barrier(jnp.mean(attention_output * attention_output, axis=-1, keepdims=True)) + EPSILON)
    gate_act = jax.nn.silu(output_gate_preactivation.astype(jnp.float32).reshape(SEQUENCE_LENGTH, ATTENTION_HEADS, DV))
    head_rows = (attention_output * inverse_rms * head_norm_gain.astype(jnp.float32) * gate_act).reshape(SEQUENCE_LENGTH, ATTENTION_HEADS * DV).astype(jnp.bfloat16)
    mid_rows = (residual.astype(jnp.float32) + jnp.dot(head_rows, output_projection, preferred_element_type=jnp.float32)).astype(jnp.bfloat16)
    mid_float = mid_rows.astype(jnp.float32)
    normed = (mid_float * lax.rsqrt(lax.optimization_barrier(jnp.mean(mid_float * mid_float, axis=-1, keepdims=True)) + EPSILON) * feedforward_gain.astype(jnp.float32)).astype(jnp.bfloat16)
    route_weight = ROUTE_SCALE * router_score / lax.optimization_barrier(jnp.sum(router_score, axis=1, keepdims=True))
    flat_expert = routing.reshape(N_SP, TOK_DEV * K)
    one_hot = (flat_expert[..., None] == jnp.arange(E, dtype=jnp.int32)).astype(jnp.int32)
    rank_before = lax.optimization_barrier(jnp.sum((jnp.cumsum(one_hot, axis=1) - one_hot) * one_hot, axis=2))
    block_index = jnp.arange(N_SP, dtype=jnp.int32)[:, None]
    table_index = (flat_expert * (N_SP * MOST) + block_index * MOST + rank_before).reshape(-1).astype(jnp.int32)
    assign_token = jnp.arange(SEQUENCE_LENGTH * K, dtype=jnp.int32) // K
    slot_token = jnp.full((E * N_SP * MOST,), SEQUENCE_LENGTH, jnp.int32).at[table_index].set(assign_token)
    slot_weight = jnp.zeros((E * N_SP * MOST,), jnp.float32).at[table_index].set(route_weight.reshape(-1))
    padded = jnp.concatenate([normed, jnp.zeros((1, D), jnp.bfloat16)], axis=0)

    def expert_rows(inputs):
        token_ids, expert_id = inputs
        first = expert_id * FF
        gate_cols = lax.dynamic_slice_in_dim(expert_gate_weight, first, FF, 1)
        up_cols = lax.dynamic_slice_in_dim(expert_up_weight, first, FF, 1)
        down_rows = lax.dynamic_slice_in_dim(expert_down_weight, first, FF, 0)
        rows_in = padded[token_ids]
        hidden = (jax.nn.silu(jnp.dot(rows_in, gate_cols, preferred_element_type=jnp.float32)) * jnp.dot(rows_in, up_cols, preferred_element_type=jnp.float32)).astype(jnp.bfloat16)
        return jnp.dot(hidden, down_rows, preferred_element_type=jnp.float32).astype(jnp.bfloat16)
    expert_out = lax.map(expert_rows, (slot_token.reshape(E, N_SP * MOST), jnp.arange(E, dtype=jnp.int32)))
    weighted = expert_out.reshape(-1, D).astype(jnp.float32) * slot_weight[:, None]
    routed = jax.ops.segment_sum(weighted, slot_token, num_segments=SEQUENCE_LENGTH + 1)[:SEQUENCE_LENGTH]
    shared_hidden = (jax.nn.silu(jnp.dot(normed, shared_expert_gate, preferred_element_type=jnp.float32)) * jnp.dot(normed, shared_expert_up, preferred_element_type=jnp.float32)).astype(jnp.bfloat16)
    shared = jnp.dot(shared_hidden, shared_expert_down, preferred_element_type=jnp.float32)
    return (mid_float + routed + shared).astype(jnp.bfloat16)
```

```python
import jax
import jax.numpy as jnp
from jax import lax
from jax.experimental import pallas as pl
from jax.experimental.pallas import tpu as pltpu
from jax.sharding import Mesh
from jax.sharding import PartitionSpec as P

DK = 128
DV = 256
BLOCK = 64
TOK = 256
MOST = 12
SLOTS = 384
D = 2048
SP = ("z", "x")
TP = ("yg", "yn", "c")
Y = ("yg", "yn")
GROUP = ("yn", "c")
F32 = jnp.float32
BF16 = jnp.bfloat16
HIGHEST = lax.Precision.HIGHEST
EPSILON = 1e-06
ROUTE_SCALE = 2.5
GATE_TEMPER = 16.0
VMEM = pl.BlockSpec(memory_space=pltpu.VMEM)
SMEM = pl.BlockSpec(memory_space=pltpu.SMEM)


def call(kernel, outs, *args, scratch=(), smem=0, flops=1000000, limit=24):
    single = not isinstance(outs, list)
    shapes = [jax.ShapeDtypeStruct(s, t) for s, t in ([outs] if single else outs)]
    got = pl.pallas_call(
        kernel,
        out_shape=shapes,
        in_specs=[SMEM] * smem + [VMEM] * (len(args) - smem),
        out_specs=[VMEM] * len(shapes),
        scratch_shapes=list(scratch),
        compiler_params=pltpu.CompilerParams(vmem_limit_bytes=limit * 2**20),
        cost_estimate=pl.CostEstimate(flops=flops, bytes_accessed=1000000, transcendentals=0),
        name=kernel.__name__,
    )(*args)
    return got[0] if single else got


def nt(a, b, **kw):
    return lax.dot_general(
        a, b, (((1,), (1,)), ((), ())), preferred_element_type=F32, **kw
    )


def decays(decay_ref, extra_ref):
    raw = decay_ref[...].astype(F32)
    logs = jax.nn.log_sigmoid(raw) / GATE_TEMPER + extra_ref[...]
    rows = lax.broadcasted_iota(jnp.int32, (BLOCK, BLOCK), 0)
    cols = lax.broadcasted_iota(jnp.int32, (BLOCK, BLOCK), 1)
    lower = (rows >= cols).astype(F32)
    inside = [
        jnp.dot(lower, logs[b * BLOCK : (b + 1) * BLOCK], precision=HIGHEST,
                preferred_element_type=F32)
        for b in range(TOK // BLOCK)
    ]
    return inside


def block_states(inside, key_ref, value_ref):
    state = jnp.zeros((DV, DK), F32)
    states = []
    total = jnp.zeros((1, DK), F32)
    for b, cum in enumerate(inside):
        states.append(state)
        rows = pl.ds(b * BLOCK, BLOCK)
        end = cum[BLOCK - 1 : BLOCK]
        key_end = key_ref[rows, :].astype(F32) * jnp.exp(end - cum)
        value = value_ref[rows, :].astype(F32)
        fresh = jnp.dot(value.T, key_end, precision=HIGHEST, preferred_element_type=F32)
        state = jnp.exp(end) * state + fresh
        total = total + end
    return states, state, total


def state_kernel(key_ref, value_ref, decay_ref, extra_ref, out_ref):
    inside = decays(decay_ref, extra_ref)
    _, state, total = block_states(inside, key_ref, value_ref)
    out_ref[:, 0:8, :] = state.reshape(32, 8, DK).astype(BF16)
    decay = jnp.exp(total)
    high = decay.astype(BF16).astype(F32)
    row = lax.broadcasted_iota(jnp.int32, (8, DK), 0)
    tail = jnp.where(row == 0, high, jnp.where(row == 1, decay - high, 0.0))
    out_ref[:, 8:16, :] = jnp.broadcast_to(tail[None], (32, 8, DK)).astype(BF16)


def scan_kernel(in_ref, out_ref):
    state = jnp.zeros((8, DK), F32)
    for s in range(32):
        out_ref[s] = state.astype(BF16)
        block = in_ref[s].astype(F32)
        decay = block[8:9] + block[9:10]
        state = decay * state + block[0:8]


def local_kernel(query_ref, key_ref, value_ref, decay_ref, extra_ref, local_ref, start_ref):
    inside = decays(decay_ref, extra_ref)
    states, _, _ = block_states(inside, key_ref, value_ref)
    rows_at = lax.broadcasted_iota(jnp.int32, (BLOCK, BLOCK), 0)
    cols_at = lax.broadcasted_iota(jnp.int32, (BLOCK, BLOCK), 1)
    before = jnp.zeros((1, DK), F32)
    for b, cum in enumerate(inside):
        rows = pl.ds(b * BLOCK, BLOCK)
        query = query_ref[rows, :].astype(F32) * DK ** (-0.5)
        key = key_ref[rows, :].astype(F32)
        value = value_ref[rows, :].astype(F32)
        query_decay = query * jnp.exp(cum)
        scores = nt(query_decay, key * jnp.exp(-cum), precision=HIGHEST)
        scores = jnp.where(rows_at >= cols_at, scores, 0.0)
        mixed = jnp.dot(scores, value, precision=HIGHEST, preferred_element_type=F32)
        if b > 0:
            mixed = mixed + nt(query_decay, states[b], precision=HIGHEST)
        local_ref[rows, :] = mixed
        start_ref[rows, :] = query * jnp.exp(cum + before)
        before = before + cum[BLOCK - 1 : BLOCK]


def head_kernel(local_ref, start_ref, enter_ref, gate_ref, gain_ref, out_ref):
    mixed = local_ref[...] + nt(start_ref[...], enter_ref[...].astype(F32), precision=HIGHEST)
    scale = lax.rsqrt(jnp.mean(mixed * mixed, axis=-1, keepdims=True) + EPSILON)
    gate = jax.nn.silu(gate_ref[...].astype(F32))
    out_ref[...] = (mixed * scale * gain_ref[...].astype(F32) * gate).astype(BF16)


def project_kernel(ids_ref, own_ref, other_ref, weight_ref, residual_ref, out_ref):
    y, c = ids_ref[0], ids_ref[1]
    mine = pl.ds(pl.multiple_of(c * DV, DV), DV)
    theirs = pl.ds(pl.multiple_of((1 - c) * DV, DV), DV)
    own, other = own_ref[...], other_ref[...]
    residual = residual_ref[...].astype(F32)
    for k in range(0, 8, 2):
        w_mine = jnp.concatenate([weight_ref[k, mine, :], weight_ref[k + 1, mine, :]], axis=1)
        w_theirs = jnp.concatenate([weight_ref[k, theirs, :], weight_ref[k + 1, theirs, :]], axis=1)
        part = jnp.dot(own, w_mine, preferred_element_type=F32)
        part = part + jnp.dot(other, w_theirs, preferred_element_type=F32)
        for j in range(2):
            slab = part[:, j * 128 : (j + 1) * 128]
            slab = slab + residual * (y == k + j).astype(F32)
            out_ref[:, k + j] = slab.reshape(8, 32, 128).astype(BF16)


def reduce_kernel(in_ref, out_ref):
    total = in_ref[0].astype(F32)
    for s in range(1, 8):
        total = total + in_ref[s].astype(F32)
    mid = total.astype(BF16)
    for dest in range(8):
        for q in range(4):
            out_ref[dest, q] = mid[2 * q + dest % 2]


def routing_kernel(ids_ref, routing_ref, score_ref, pick_ref, high_ref, low_ref):
    group = ids_ref[2]
    experts = lax.broadcasted_iota(jnp.int32, (TOK, 128), 1)
    hot = [(routing_ref[:, k : k + 1] == experts).astype(F32) for k in range(4)]
    named = hot[0] + hot[1] + hot[2] + hot[3]
    rows = lax.broadcasted_iota(jnp.int32, (TOK, TOK), 0)
    cols = lax.broadcasted_iota(jnp.int32, (TOK, TOK), 1)
    earlier = (rows > cols).astype(BF16)
    ranks = jnp.dot(earlier, named.astype(BF16), preferred_element_type=F32)
    scores = [score_ref[:, k : k + 1] for k in range(4)]
    total = scores[0] + scores[1] + scores[2] + scores[3]
    slots = lax.broadcasted_iota(jnp.int32, (TOK, SLOTS), 1)
    picked = jnp.zeros((TOK, SLOTS), F32)
    weighted = jnp.zeros((TOK, SLOTS), F32)
    for k in range(4):
        expert = routing_ref[:, k : k + 1]
        rank = jnp.sum(hot[k] * ranks, axis=1, keepdims=True).astype(jnp.int32)
        place = lax.shift_right_logical(expert, 2) * MOST + rank
        place = jnp.where((expert & 3) == group, place, -1)
        here = (place == slots).astype(F32)
        picked = picked + here
        weighted = weighted + here * (ROUTE_SCALE * scores[k] / total)
    pick_ref[...] = picked.T.astype(BF16)
    high = weighted.astype(BF16)
    high_ref[...] = high
    low_ref[...] = (weighted - high.astype(F32)).astype(BF16)


def dispatch_kernel(pick_ref, mid_ref, out_ref, wide_ref):
    pick = pick_ref[...]
    for q in range(4):
        tile = mid_ref[:, q].reshape(TOK, 128)
        wide_ref[pl.ds(q, SLOTS, stride=4), :] = jnp.dot(pick, tile, preferred_element_type=F32)
    out_ref[...] = wide_ref[...].astype(BF16)


def expert_kernel(ids_ref, x0, x1, x2, x3, gate_ref, up_ref, gain_ref, out_ref, wide_ref, rows_ref):
    part = ids_ref[3]
    squares = jnp.zeros((SLOTS, 128), F32)
    for m, x_ref in enumerate((x0, x1, x2, x3)):
        wide_ref[...] = x_ref[...].astype(F32)
        for q in range(4):
            slab = q * 4 + (part ^ m)
            tile = wide_ref[pl.ds(q, SLOTS, stride=4), :]
            squares = squares + tile * tile
            scaled = (tile * gain_ref[pl.ds(slab, 1), :]).astype(BF16)
            rows_ref[:, pl.ds(pl.multiple_of(slab * 128, 128), 128)] = scaled
    scale = lax.rsqrt(jnp.sum(squares, axis=1, keepdims=True) * (1.0 / D) + EPSILON)
    gate = jnp.dot(rows_ref[...], gate_ref[...], preferred_element_type=F32) * scale
    up = jnp.dot(rows_ref[...], up_ref[...], preferred_element_type=F32) * scale
    out_ref[...] = (jax.nn.silu(gate) * up).astype(BF16)


def down_kernel(ids_ref, h0, h1, h2, h3, down_ref, out_ref, wide_ref):
    part = ids_ref[3]
    total = jnp.dot(h0[...], down_ref[part], preferred_element_type=F32)
    for m, h_ref in ((1, h1), (2, h2), (3, h3)):
        total = total + jnp.dot(h_ref[...], down_ref[part ^ m], preferred_element_type=F32)
    for q in range(4):
        wide_ref[pl.ds(q, SLOTS, stride=4), :] = total[:, q * 128 : (q + 1) * 128]
    out_ref[...] = wide_ref[...].astype(BF16)


def shared_in_kernel(ids_ref, mid_ref, weight_ref, gain_ref, out_ref):
    part = ids_ref[3]
    squares = jnp.zeros((TOK, 128), F32)
    pre = jnp.zeros((TOK, 256), F32)
    for q in range(4):
        tile = mid_ref[:, q].reshape(TOK, 128).astype(F32)
        squares = squares + tile * tile
        scaled = (tile * gain_ref[pl.ds(q * 4 + part, 1), :]).astype(BF16)
        weight = jnp.concatenate(
            [weight_ref[p, q, 0:32, :] for p in range(4)]
            + [weight_ref[p, q, 32:64, :] for p in range(4)],
            axis=0,
        )
        pre = pre + nt(scaled, weight)
    out_ref[:, 0:256] = pre.astype(BF16)
    ssq = jnp.sum(squares, axis=1, keepdims=True)
    high = ssq.astype(BF16).astype(F32)
    lane = lax.broadcasted_iota(jnp.int32, (TOK, 128), 1)
    tail = jnp.where(lane == 0, high, jnp.where(lane == 1, ssq - high, 0.0))
    out_ref[:, 256:384] = tail.astype(BF16)


def shared_hidden_kernel(in_ref, out_ref):
    total = in_ref[0].astype(F32)
    for s in range(1, 4):
        total = total + in_ref[s].astype(F32)
    ssq = jnp.sum(total[:, 256:384], axis=1, keepdims=True)
    scale = lax.rsqrt(ssq * (1.0 / D) + EPSILON)
    hidden = jax.nn.silu(total[:, 0:128] * scale) * (total[:, 128:256] * scale)
    hidden = hidden.astype(BF16)
    for dest in range(4):
        out_ref[dest] = hidden


def combine_kernel(back_ref, high_ref, low_ref, hidden_ref, down_ref, out_ref, wide_ref):
    wide_ref[...] = back_ref[...].astype(F32)
    hidden = hidden_ref[...].reshape(TOK, 128)
    for q in range(4):
        tile = wide_ref[pl.ds(q, SLOTS, stride=4), :].astype(BF16)
        total = jnp.dot(high_ref[...], tile, preferred_element_type=F32)
        total = total + jnp.dot(low_ref[...], tile, preferred_element_type=F32)
        total = total + jnp.dot(hidden, down_ref[q], preferred_element_type=F32)
        out_ref[q] = total.astype(BF16)


def final_kernel(ids_ref, in_ref, mid_ref, out_ref):
    group = ids_ref[2]
    total = mid_ref[:, group].reshape(TOK, 128).astype(F32)
    for s in range(4):
        total = total + in_ref[s].astype(F32)
    out_ref[...] = total.astype(BF16)


def exchange(value, axes):
    return lax.all_to_all(value, axes, split_axis=0, concat_axis=0, tiled=True)


def swapped(value, axis):
    return lax.ppermute(value, axis, [(0, 1), (1, 0)])


def body(
    queries,
    key_matrix,
    value_matrix,
    output_gate_preactivation,
    decay_preactivation,
    extra_log_decay,
    head_norm_gain,
    output_projection,
    residual,
    feedforward_gain,
    routing,
    router_score,
    expert_gate_weight,
    expert_up_weight,
    expert_down_weight,
    shared_expert_gate,
    shared_expert_up,
    shared_expert_down,
):
    y, c, g, p = (lax.axis_index(a) for a in (Y, "c", "yg", GROUP))
    ids = jnp.stack([y, c, g, p]).astype(jnp.int32)
    gain = feedforward_gain.astype(F32).reshape(16, 128)
    head_gain = head_norm_gain.reshape(1, DV)

    payload = call(
        state_kernel, ((32, 16, DK), BF16),
        key_matrix, value_matrix, decay_preactivation, extra_log_decay,
    )
    weights = exchange(output_projection.reshape(8, 512, 128), Y)
    payload, down, gate_t, up_t, shared_down = lax.optimization_barrier(
        (payload, expert_down_weight, shared_expert_gate, shared_expert_up, shared_expert_down)
    )
    states = exchange(payload, SP)
    local, start = call(
        local_kernel, [((TOK, DV), F32), ((TOK, DK), F32)],
        queries, key_matrix, value_matrix, decay_preactivation, extra_log_decay,
    )
    down = exchange(
        down.reshape(256, 4, 4, 128).transpose(2, 0, 1, 3).reshape(4, 256, 512), GROUP
    )
    shared_in = jnp.concatenate(
        [w.T.reshape(32, 4, 4, 128).transpose(2, 1, 0, 3) for w in (gate_t, up_t)], axis=2
    )
    shared_in = exchange(shared_in, GROUP)
    shared_down = exchange(shared_down.reshape(4, 128, 128), "yg")
    pick, high, low = call(
        routing_kernel,
        [((SLOTS, TOK), BF16), ((TOK, SLOTS), BF16), ((TOK, SLOTS), BF16)],
        ids, routing, router_score, smem=1,
    )

    entering = exchange(call(scan_kernel, ((32, 8, DK), BF16), states), SP).reshape(DV, DK)
    head_rows = call(
        head_kernel, ((TOK, DV), BF16),
        local, start, entering, output_gate_preactivation, head_gain,
    )
    partial = call(
        project_kernel, ((8, 8, 32, 128), BF16),
        ids, head_rows, swapped(head_rows, "c"), weights, residual, smem=1,
    )
    mid_send = call(reduce_kernel, ((8, 4, 32, 128), BF16), exchange(partial, Y))
    mid = exchange(mid_send, Y)

    outgoing = call(
        dispatch_kernel, ((4 * SLOTS, 128), BF16), pick, mid,
        scratch=[pltpu.VMEM((4 * SLOTS, 128), F32)],
    )
    own = exchange(outgoing.reshape(32, 48, 128), SP).reshape(4 * SLOTS, 128)

    pre = call(
        shared_in_kernel, ((TOK, 384), BF16), ids, mid, shared_in, gain, smem=1,
    )
    hidden = call(
        shared_hidden_kernel, ((4, 64, 128), BF16), exchange(pre.reshape(4, 64, 384), GROUP)
    )
    hidden = exchange(hidden, GROUP)

    across = swapped(own, "yn")
    beside = swapped(own, "c")
    rows_far = swapped(across, "c")
    routed = call(
        expert_kernel, ((SLOTS, 256), BF16),
        ids, own, beside, across, rows_far, expert_gate_weight, expert_up_weight, gain,
        smem=1,
        scratch=[pltpu.VMEM((4 * SLOTS, 128), F32), pltpu.VMEM((SLOTS, D), BF16)],
    )
    routed_across = swapped(routed, "yn")
    routed_beside = swapped(routed, "c")
    routed_far = swapped(routed_across, "c")
    expert_out = call(
        down_kernel, ((4 * SLOTS, 128), BF16),
        ids, routed, routed_beside, routed_across, routed_far, down,
        smem=1, scratch=[pltpu.VMEM((4 * SLOTS, 128), F32)],
    )
    back = exchange(expert_out.reshape(32, 48, 128), SP).reshape(4 * SLOTS, 128)
    sums = call(
        combine_kernel, ((4, TOK, 128), BF16),
        back, high, low, hidden, shared_down,
        scratch=[pltpu.VMEM((4 * SLOTS, 128), F32)],
    )
    return call(final_kernel, ((TOK, 128), BF16), ids, exchange(sums, "yg"), mid, smem=1)


def solution(mesh):
    finer = Mesh(mesh.devices.reshape(8, 4, 4, 2, 2), ("z", "x", "yg", "yn", "c"))
    in_specs = (
        P(SP, TP),
        P(SP, TP),
        P(SP, TP),
        P(SP, TP),
        P(SP, TP),
        P(SP, TP),
        P(),
        P(None, TP),
        P(SP, TP),
        P(),
        P(SP, None),
        P(SP, None),
        P(None, SP + TP),
        P(None, SP + TP),
        P(SP + TP, None),
        P(None, TP),
        P(None, TP),
        P(None, TP),
    )
    return jax.shard_map(
        body, mesh=finer, in_specs=in_specs, out_specs=P(SP, TP), check_vma=False
    )
```

```python
import jax
import jax.numpy as jnp
from jax import lax
from jax.experimental import pallas as pl
from jax.experimental.pallas import tpu as pltpu
from jax.sharding import Mesh
from jax.sharding import PartitionSpec as P

DK = 128
DV = 256
BLOCK = 64
TOK = 256
MOST = 12
SLOTS = 384
ALL_SLOTS = 1536
PITCH = 56
D = 2048
SP = ("z", "x")
SPG = ("z", "x", "yg")
TP = ("yg", "yn", "c")
GROUP = ("yn", "c")
F32 = jnp.float32
BF16 = jnp.bfloat16
HIGHEST = lax.Precision.HIGHEST
EPSILON = 1e-06
ROUTE_SCALE = 2.5
GATE_TEMPER = 16.0
VMEM = pl.BlockSpec(memory_space=pltpu.VMEM)
SMEM = pl.BlockSpec(memory_space=pltpu.SMEM)


def call(kernel, outs, *args, scratch=(), smem=0, limit=24):
    single = not isinstance(outs, list)
    shapes = [jax.ShapeDtypeStruct(s, t) for s, t in ([outs] if single else outs)]
    got = pl.pallas_call(
        kernel,
        out_shape=shapes,
        in_specs=[SMEM] * smem + [VMEM] * (len(args) - smem),
        out_specs=[VMEM] * len(shapes),
        scratch_shapes=list(scratch),
        compiler_params=pltpu.CompilerParams(vmem_limit_bytes=limit * 2**20),
        cost_estimate=pl.CostEstimate(
            flops=1000000, bytes_accessed=1000000, transcendentals=0
        ),
    )(*args)
    return got[0] if single else got


def nt(a, b, **kw):
    return lax.dot_general(
        a, b, (((1,), (1,)), ((), ())), preferred_element_type=F32, **kw
    )


def decays(decay_ref, extra_ref):
    raw = decay_ref[...].astype(F32)
    logs = jax.nn.log_sigmoid(raw) / GATE_TEMPER + extra_ref[...]
    rows = lax.broadcasted_iota(jnp.int32, (BLOCK, BLOCK), 0)
    cols = lax.broadcasted_iota(jnp.int32, (BLOCK, BLOCK), 1)
    lower = (rows >= cols).astype(F32)
    inside = [
        jnp.dot(lower, logs[b * BLOCK : (b + 1) * BLOCK], precision=HIGHEST,
                preferred_element_type=F32)
        for b in range(TOK // BLOCK)
    ]
    return inside


def block_states(inside, key_ref, value_ref):
    state = jnp.zeros((DV, DK), F32)
    states = []
    total = jnp.zeros((1, DK), F32)
    for b, cum in enumerate(inside):
        states.append(state)
        rows = pl.ds(b * BLOCK, BLOCK)
        end = cum[BLOCK - 1 : BLOCK]
        key_end = key_ref[rows, :].astype(F32) * jnp.exp(end - cum)
        value = value_ref[rows, :].astype(F32)
        fresh = jnp.dot(value.T, key_end, precision=HIGHEST, preferred_element_type=F32)
        state = jnp.exp(end) * state + fresh
        total = total + end
    return states, state, total


def state_kernel(key_ref, value_ref, decay_ref, extra_ref, out_ref):
    inside = decays(decay_ref, extra_ref)
    _, state, total = block_states(inside, key_ref, value_ref)
    out_ref[:, 0:8, :] = state.reshape(32, 8, DK).astype(BF16)
    decay = jnp.exp(total)
    high = decay.astype(BF16).astype(F32)
    row = lax.broadcasted_iota(jnp.int32, (8, DK), 0)
    tail = jnp.where(row == 0, high, jnp.where(row == 1, decay - high, 0.0))
    out_ref[:, 8:16, :] = jnp.broadcast_to(tail[None], (32, 8, DK)).astype(BF16)


def scan_kernel(in_ref, out_ref):
    state = jnp.zeros((8, DK), F32)
    for s in range(32):
        out_ref[s] = state.astype(BF16)
        block = in_ref[s].astype(F32)
        decay = block[8:9] + block[9:10]
        state = decay * state + block[0:8]


def local_kernel(query_ref, key_ref, value_ref, decay_ref, extra_ref, local_ref, start_ref):
    inside = decays(decay_ref, extra_ref)
    states, _, _ = block_states(inside, key_ref, value_ref)
    rows_at = lax.broadcasted_iota(jnp.int32, (BLOCK, BLOCK), 0)
    cols_at = lax.broadcasted_iota(jnp.int32, (BLOCK, BLOCK), 1)
    before = jnp.zeros((1, DK), F32)
    for b, cum in enumerate(inside):
        rows = pl.ds(b * BLOCK, BLOCK)
        query = query_ref[rows, :].astype(F32) * DK ** (-0.5)
        key = key_ref[rows, :].astype(F32)
        value = value_ref[rows, :].astype(F32)
        query_decay = query * jnp.exp(cum)
        scores = nt(query_decay, key * jnp.exp(-cum), precision=HIGHEST)
        scores = jnp.where(rows_at >= cols_at, scores, 0.0)
        mixed = jnp.dot(scores, value, precision=HIGHEST, preferred_element_type=F32)
        if b > 0:
            mixed = mixed + nt(query_decay, states[b], precision=HIGHEST)
        local_ref[rows, :] = mixed
        start_ref[rows, :] = query * jnp.exp(cum + before)
        before = before + cum[BLOCK - 1 : BLOCK]


def head_kernel(local_ref, start_ref, enter_ref, gate_ref, gain_ref, out_ref):
    mixed = local_ref[...] + nt(start_ref[...], enter_ref[...].astype(F32), precision=HIGHEST)
    scale = lax.rsqrt(jnp.mean(mixed * mixed, axis=-1, keepdims=True) + EPSILON)
    gate = jax.nn.silu(gate_ref[...].astype(F32))
    rows = (mixed * scale * gain_ref[...].astype(F32) * gate).astype(BF16)
    for dest in range(4):
        out_ref[dest] = rows


def project_kernel(ids_ref, heads_ref, w0, w1, w2, w3, out_ref):
    part = ids_ref[0]
    for m in (0, 2):
        pair = ((w0, w1), None, (w2, w3))[m]
        total = jnp.zeros((TOK, 256), F32)
        for h in range(4):
            lanes = slice(h * 128, (h + 1) * 128)
            weight = jnp.concatenate([w[0:256, lanes] for w in pair], axis=1)
            total = total + jnp.dot(heads_ref[h], weight, preferred_element_type=F32)
        out_ref[part ^ m] = total[:, :128].astype(BF16)
        out_ref[part ^ (m + 1)] = total[:, 128:].astype(BF16)


def places(routing_ref):
    experts = lax.broadcasted_iota(jnp.int32, (TOK, 128), 1)
    hot = [(routing_ref[:, k : k + 1] == experts).astype(F32) for k in range(4)]
    named = hot[0] + hot[1] + hot[2] + hot[3]
    rows = lax.broadcasted_iota(jnp.int32, (TOK, TOK), 0)
    cols = lax.broadcasted_iota(jnp.int32, (TOK, TOK), 1)
    earlier = (rows > cols).astype(BF16)
    ranks = jnp.dot(earlier, named.astype(BF16), preferred_element_type=F32)
    return [
        routing_ref[:, k : k + 1] * MOST
        + jnp.sum(hot[k] * ranks, axis=1, keepdims=True).astype(jnp.int32)
        for k in range(4)
    ]


def pick_kernel(routing_ref, pick_ref):
    place = places(routing_ref)
    slots = lax.broadcasted_iota(jnp.int32, (TOK, 512), 1)
    for j in range(ALL_SLOTS // 512):
        picked = jnp.zeros((TOK, 512), F32)
        for k in range(4):
            picked = picked + (place[k] - j * 512 == slots).astype(F32)
        pick_ref[j * 512 : (j + 1) * 512, :] = picked.T.astype(BF16)


def weigh_kernel(routing_ref, score_ref, high_ref, low_ref):
    place = places(routing_ref)
    scores = [score_ref[:, k : k + 1] for k in range(4)]
    total = scores[0] + scores[1] + scores[2] + scores[3]
    slots = lax.broadcasted_iota(jnp.int32, (TOK, 512), 1)
    for j in range(ALL_SLOTS // 512):
        weighted = jnp.zeros((TOK, 512), F32)
        for k in range(4):
            here = (place[k] - j * 512 == slots).astype(F32)
            weighted = weighted + here * (ROUTE_SCALE * scores[k] / total)
        high = weighted.astype(BF16)
        high_ref[:, j * 512 : (j + 1) * 512] = high
        low_ref[:, j * 512 : (j + 1) * 512] = (weighted - high.astype(F32)).astype(BF16)


def dispatch_kernel(pick_ref, in_ref, residual_ref, out_ref, mid_ref):
    total = residual_ref[...].astype(F32)
    for s in range(4):
        total = total + in_ref[s].astype(F32)
    mid = total.astype(BF16)
    mid_ref[...] = mid
    for j in range(4):
        rows = pl.ds(j * SLOTS, SLOTS)
        picked = jnp.dot(pick_ref[rows, :], mid, preferred_element_type=F32)
        out_ref[rows, :] = picked.astype(BF16)


def expert_kernel(ids_ref, x0, x1, x2, x3, gate_ref, up_ref, gain_ref, out_ref, wide_ref, rows_ref):
    part = ids_ref[0]
    squares = jnp.zeros((SLOTS, 128), F32)
    for m, x_ref in enumerate((x0, x1, x2, x3)):
        for s in range(32):
            wide_ref[m, s * PITCH : s * PITCH + 48, :] = x_ref[s * 48 : (s + 1) * 48, :].astype(F32)
    for m in range(4):
        for q in range(4):
            slab = q * 4 + (part ^ m)
            tile = jnp.concatenate(
                [wide_ref[m, pl.ds(q * MOST + r, 32, stride=PITCH), :] for r in range(MOST)], axis=0
            )
            squares = squares + tile * tile
            scaled = (tile * gain_ref[pl.ds(slab, 1), :]).astype(BF16)
            rows_ref[:, pl.ds(pl.multiple_of(slab * 128, 128), 128)] = scaled
    scale = lax.rsqrt(jnp.sum(squares, axis=1, keepdims=True) * (1.0 / D) + EPSILON)
    gate = jnp.dot(rows_ref[...], gate_ref[...], preferred_element_type=F32) * scale
    up = jnp.dot(rows_ref[...], up_ref[...], preferred_element_type=F32) * scale
    out_ref[...] = (jax.nn.silu(gate) * up).astype(BF16)


def down_kernel(h0, h1, h2, h3, d0, d1, d2, d3, out_ref, wide_ref):
    total = jnp.zeros((SLOTS, 512), F32)
    for h_ref, d_ref in ((h0, d0), (h1, d1), (h2, d2), (h3, d3)):
        total = total + jnp.dot(h_ref[...], d_ref[256:512, :], preferred_element_type=F32)
    for q in range(4):
        for r in range(MOST):
            wide_ref[pl.ds(q * MOST + r, 32, stride=PITCH), :] = total[
                r * 32 : (r + 1) * 32, q * 128 : (q + 1) * 128
            ]
    for s in range(32):
        out_ref[s * 48 : (s + 1) * 48, :] = wide_ref[s * PITCH : s * PITCH + 48, :].astype(BF16)


def parts_kernel(ids_ref, project_ref, down_ref, shared_ref, *out_refs):
    part = ids_ref[0]
    for m, out_ref in enumerate(out_refs):
        for q in range(4):
            slab = q * 4 + (part ^ m)
            lanes = slice(q * 128, (q + 1) * 128)
            out_ref[0:256, lanes] = project_ref[pl.ds(pl.multiple_of(slab * 256, 256), 256), :]
            columns = pl.ds(pl.multiple_of(slab * 128, 128), 128)
            out_ref[256:512, lanes] = down_ref[:, columns]
            out_ref[512:576, lanes] = shared_ref[:, columns]


def shared_in_kernel(ids_ref, m0, m1, m2, m3, w0, w1, w2, w3, gain_ref, out_ref, weight_ref, mid_ref):
    part, group = ids_ref[0], ids_ref[1]
    for m, w_ref in enumerate((w0, w1, w2, w3)):
        at = (part ^ m) * 32
        weight_ref[pl.ds(pl.multiple_of(at, 32), 32), :] = w_ref[512:544, :]
        weight_ref[pl.ds(pl.multiple_of(at + 128, 32), 32), :] = w_ref[544:576, :]
    for d, m_ref in enumerate((m0, m1, m2, m3)):
        mid_ref[(group - d) & 3] = m_ref[...]
    squares = jnp.zeros((TOK, 128), F32)
    pre = jnp.zeros((TOK, 256), F32)
    for q in range(4):
        tile = mid_ref[q].astype(F32)
        squares = squares + tile * tile
        scaled = (tile * gain_ref[pl.ds(q * 4 + part, 1), :]).astype(BF16)
        pre = pre + nt(scaled, weight_ref[:, q * 128 : (q + 1) * 128])
    ssq = jnp.sum(squares, axis=1, keepdims=True)
    high = ssq.astype(BF16).astype(F32)
    lane = lax.broadcasted_iota(jnp.int32, (TOK, 128), 1)
    tail = jnp.where(lane == 0, high, jnp.where(lane == 1, ssq - high, 0.0)).astype(BF16)
    pre = pre.astype(BF16)
    for dest in range(4):
        out_ref[dest, :, 0:256] = pre
        out_ref[dest, :, 256:384] = tail


def shared_hidden_kernel(in_ref, out_ref):
    total = sum(in_ref[s].astype(F32) for s in range(4))
    ssq = jnp.sum(total[:, 256:384], axis=1, keepdims=True)
    scale = lax.rsqrt(ssq * (1.0 / D) + EPSILON)
    hidden = jax.nn.silu(total[:, 0:128] * scale) * (total[:, 128:256] * scale)
    out_ref[...] = hidden.astype(BF16)


def final_kernel(ids_ref, back_ref, high_ref, low_ref, h0, h1, h2, h3, down_ref, mid_ref, out_ref):
    group = ids_ref[1]
    back = back_ref[...]
    total = mid_ref[...].astype(F32)
    total = total + jnp.dot(high_ref[...], back, preferred_element_type=F32)
    total = total + jnp.dot(low_ref[...], back, preferred_element_type=F32)
    for d, h in enumerate((h0, h1, h2, h3)):
        at = pl.multiple_of(((group - d) & 3) * 128, 128)
        total = total + jnp.dot(
            h[...], down_ref[pl.ds(at, 128), :], preferred_element_type=F32
        )
    out_ref[...] = total.astype(BF16)


def exchange(value, axes):
    return lax.all_to_all(value, axes, split_axis=0, concat_axis=0, tiled=True)


def moved(value, axes, target):
    count = lax.axis_size(axes)
    return lax.ppermute(value, axes, [(i, target(i) % count) for i in range(count)])


def shifted(values, axes):
    return [moved(v, axes, lambda i, d=d: i + d) for d, v in enumerate(values, 1)]


def swapped(value, axis):
    return moved(value, axis, lambda i: i ^ 1)


def grouped(values):
    return [moved(v, GROUP, lambda i, m=m: i ^ m) for m, v in enumerate(values, 1)]


def body(
    queries,
    key_matrix,
    value_matrix,
    output_gate_preactivation,
    decay_preactivation,
    extra_log_decay,
    head_norm_gain,
    output_projection,
    residual,
    feedforward_gain,
    routing,
    router_score,
    expert_gate_weight,
    expert_up_weight,
    expert_down_weight,
    shared_expert_gate,
    shared_expert_up,
    shared_expert_down,
):
    ids = jnp.stack([lax.axis_index(a) for a in (GROUP, "yg")]).astype(jnp.int32)
    gain = feedforward_gain.astype(F32).reshape(16, 128)
    head_gain = head_norm_gain.reshape(1, DV)

    payload = call(
        state_kernel, ((32, 16, DK), BF16),
        key_matrix, value_matrix, decay_preactivation, extra_log_decay,
    )
    states = exchange(payload, SP)
    local, start = call(
        local_kernel, [((TOK, DV), F32), ((TOK, DK), F32)],
        queries, key_matrix, value_matrix, decay_preactivation, extra_log_decay,
    )
    pick = call(pick_kernel, ((ALL_SLOTS, TOK), BF16), routing)
    high, low = call(
        weigh_kernel, [((TOK, ALL_SLOTS), BF16), ((TOK, ALL_SLOTS), BF16)], routing, router_score
    )
    shared_in = jnp.concatenate([shared_expert_gate.T, shared_expert_up.T], axis=0)
    own_part, *far_parts = call(
        parts_kernel, [((576, 512), BF16)] * 4,
        ids, output_projection, expert_down_weight, shared_in, smem=1,
    )
    parts = [own_part] + grouped(far_parts)

    entering = exchange(call(scan_kernel, ((32, 8, DK), BF16), states), SP)
    head_rows = call(
        head_kernel, ((4, TOK, DV), BF16),
        local, start, entering.reshape(DV, DK), output_gate_preactivation, head_gain,
    )
    partial = call(
        project_kernel, ((4, TOK, 128), BF16),
        ids, exchange(head_rows, "yg"), *parts, smem=1,
    )
    outgoing, mid = call(
        dispatch_kernel, [((ALL_SLOTS, 128), BF16), ((TOK, 128), BF16)],
        pick, exchange(partial, GROUP), residual,
    )
    own = exchange(outgoing.reshape(128, 3, 4, 128), SPG).reshape(ALL_SLOTS, 128)
    mids = [mid] + shifted([mid] * 3, "yg")

    across = swapped(own, "yn")
    beside = swapped(own, "c")
    far = swapped(across, "c")
    pre = call(
        shared_in_kernel, ((4, TOK, 384), BF16), ids, *mids, *parts, gain, smem=1,
        scratch=[pltpu.VMEM((256, 512), BF16), pltpu.VMEM((4, TOK, 128), BF16)],
    )
    pre = exchange(pre, GROUP)
    routed = call(
        expert_kernel, ((SLOTS, 256), BF16),
        ids, own, beside, across, far, expert_gate_weight, expert_up_weight, gain,
        smem=1,
        scratch=[pltpu.VMEM((4, 32 * PITCH, 128), F32), pltpu.VMEM((SLOTS, D), BF16)],
    )
    routed_across = swapped(routed, "yn")
    routed_beside = swapped(routed, "c")
    routed_far = swapped(routed_across, "c")
    expert_out = call(
        down_kernel, ((ALL_SLOTS, 128), BF16),
        routed, routed_beside, routed_across, routed_far, *parts,
        scratch=[pltpu.VMEM((32 * PITCH, 128), F32)],
    )
    back = exchange(expert_out.reshape(128, 3, 4, 128), SPG).reshape(ALL_SLOTS, 128)
    hidden = call(shared_hidden_kernel, ((TOK, 128), BF16), pre)
    hidden = [hidden] + shifted([hidden] * 3, "yg")
    return call(
        final_kernel, ((TOK, 128), BF16),
        ids, back, high, low, *hidden, shared_expert_down, mid, smem=1,
    )


def solution(mesh):
    finer = Mesh(mesh.devices.reshape(8, 4, 4, 2, 2), ("z", "x", "yg", "yn", "c"))
    in_specs = (
        P(SP, TP),
        P(SP, TP),
        P(SP, TP),
        P(SP, TP),
        P(SP, TP),
        P(SP, TP),
        P(),
        P(None, TP),
        P(SP, TP),
        P(),
        P(SP, None),
        P(SP, None),
        P(None, SP + TP),
        P(None, SP + TP),
        P(SP + TP, None),
        P(None, TP),
        P(None, TP),
        P(None, TP),
    )
    return jax.shard_map(body, mesh=finer, in_specs=in_specs, out_specs=P(SP, TP), check_vma=False)
```

```python
import jax
import jax.numpy as jnp
from jax import lax
from jax.experimental import pallas as pl
from jax.experimental.pallas import tpu as pltpu
from jax.sharding import Mesh
from jax.sharding import PartitionSpec as P

DK = 128
DV = 256
BLOCK = 64
TOK = 256
MOST = 12
SLOTS = 384
ALL_SLOTS = 1536
PITCH = 56
D = 2048
SP = ("z", "x")
SPG = ("z", "x", "yg")
TP = ("yg", "yn", "c")
GROUP = ("yn", "c")
F32 = jnp.float32
BF16 = jnp.bfloat16
HIGHEST = lax.Precision.HIGHEST
EPSILON = 1e-06
ROUTE_SCALE = 2.5
GATE_TEMPER = 16.0
VMEM = pl.BlockSpec(memory_space=pltpu.VMEM)
SMEM = pl.BlockSpec(memory_space=pltpu.SMEM)


def call(kernel, outs, *args, scratch=(), smem=0, fetch=(), late=False, limit=24):
    single = not isinstance(outs, list)
    shapes = [jax.ShapeDtypeStruct(s, t) for s, t in ([outs] if single else outs)]
    n_in, n_out, n_scratch, n_fetch = len(args), len(shapes), len(scratch), len(fetch)
    kept = n_in - n_fetch
    buffers = []
    for arg, rows in zip(args[kept:], fetch, strict=True):
        buffers.append(pltpu.VMEM((rows[1], *arg.shape[1:]), arg.dtype))

    def fetching(*refs):
        sources, results = refs[kept:n_in], refs[n_in : n_in + n_out]
        own = refs[n_in + n_out : n_in + n_out + n_scratch]
        held, sems = refs[n_in + n_out + n_scratch : -1], refs[-1]
        copies = [
            pltpu.make_async_copy(src.at[pl.ds(rows[0], rows[1])], dst, sems.at[i])
            for i, (src, dst, rows) in enumerate(zip(sources, held, fetch, strict=True))
        ]
        for copy in copies:
            copy.start()

        def ready():
            for copy in copies:
                copy.wait()

        if late:
            kernel(ready, *refs[:kept], *held, *results, *own)
        else:
            ready()
            kernel(*refs[:kept], *held, *results, *own)

    extra = buffers + [pltpu.SemaphoreType.DMA((n_fetch,))] if fetch else []
    any_spec = pl.BlockSpec(memory_space=pl.ANY)
    got = pl.pallas_call(
        fetching if fetch else kernel,
        out_shape=shapes,
        in_specs=[SMEM] * smem + [VMEM] * (kept - smem) + [any_spec] * n_fetch,
        out_specs=[VMEM] * n_out,
        scratch_shapes=list(scratch) + extra,
        compiler_params=pltpu.CompilerParams(vmem_limit_bytes=limit * 2**20),
        cost_estimate=pl.CostEstimate(
            flops=1000000, bytes_accessed=1000000, transcendentals=0
        ),
    )(*args)
    return got[0] if single else got


def nt(a, b, **kw):
    return lax.dot_general(
        a, b, (((1,), (1,)), ((), ())), preferred_element_type=F32, **kw
    )


def decays(decay_ref, extra_ref):
    raw = decay_ref[...].astype(F32)
    logs = jax.nn.log_sigmoid(raw) / GATE_TEMPER
    rows = lax.broadcasted_iota(jnp.int32, (BLOCK, BLOCK), 0)
    cols = lax.broadcasted_iota(jnp.int32, (BLOCK, BLOCK), 1)
    lower = (rows >= cols).astype(F32)
    wide_rows = lax.broadcasted_iota(jnp.int32, (BLOCK, 128), 0)
    wide_cols = lax.broadcasted_iota(jnp.int32, (BLOCK, 128), 1)
    ones = jnp.ones((128, DK), F32)
    inside = []
    for b in range(TOK // BLOCK):
        at = wide_cols - (b % 2) * BLOCK
        extra = jnp.where((at >= 0) & (at <= wide_rows), extra_ref[b // 2 : b // 2 + 1, :], 0.0)
        inside.append(
            jnp.dot(lower, logs[b * BLOCK : (b + 1) * BLOCK], precision=HIGHEST,
                    preferred_element_type=F32)
            + jnp.dot(extra, ones, precision=HIGHEST, preferred_element_type=F32)
        )
    return inside


def block_states(inside, key_ref, value_ref):
    state = jnp.zeros((DV, DK), F32)
    states = []
    total = jnp.zeros((1, DK), F32)
    for b, cum in enumerate(inside):
        states.append(state)
        rows = pl.ds(b * BLOCK, BLOCK)
        end = cum[BLOCK - 1 : BLOCK]
        key_end = key_ref[rows, :].astype(F32) * jnp.exp(end - cum)
        value = value_ref[rows, :].astype(F32)
        fresh = jnp.dot(value.T, key_end, precision=HIGHEST, preferred_element_type=F32)
        state = jnp.exp(end) * state + fresh
        total = total + end
    return states, state, total


def state_kernel(key_ref, value_ref, decay_ref, extra_ref, out_ref):
    inside = decays(decay_ref, extra_ref)
    _, state, total = block_states(inside, key_ref, value_ref)
    out_ref[:, 0:8, :] = state.reshape(32, 8, DK).astype(BF16)
    decay = jnp.exp(total)
    high = decay.astype(BF16).astype(F32)
    row = lax.broadcasted_iota(jnp.int32, (8, DK), 0)
    tail = jnp.where(row == 0, high, jnp.where(row == 1, decay - high, 0.0))
    out_ref[:, 8:16, :] = jnp.broadcast_to(tail[None], (32, 8, DK)).astype(BF16)


def scan_kernel(in_ref, out_ref):
    state = jnp.zeros((8, DK), F32)
    for s in range(32):
        out_ref[s] = state.astype(BF16)
        block = in_ref[s].astype(F32)
        decay = block[8:9] + block[9:10]
        state = decay * state + block[0:8]


def local_kernel(query_ref, key_ref, value_ref, decay_ref, extra_ref, local_ref, start_ref):
    inside = decays(decay_ref, extra_ref)
    states, _, _ = block_states(inside, key_ref, value_ref)
    rows_at = lax.broadcasted_iota(jnp.int32, (BLOCK, BLOCK), 0)
    cols_at = lax.broadcasted_iota(jnp.int32, (BLOCK, BLOCK), 1)
    before = jnp.zeros((1, DK), F32)
    for b, cum in enumerate(inside):
        rows = pl.ds(b * BLOCK, BLOCK)
        query = query_ref[rows, :].astype(F32) * DK ** (-0.5)
        key = key_ref[rows, :].astype(F32)
        value = value_ref[rows, :].astype(F32)
        query_decay = query * jnp.exp(cum)
        scores = nt(query_decay, key * jnp.exp(-cum), precision=HIGHEST)
        scores = jnp.where(rows_at >= cols_at, scores, 0.0)
        mixed = jnp.dot(scores, value, precision=HIGHEST, preferred_element_type=F32)
        if b > 0:
            mixed = mixed + nt(query_decay, states[b], precision=HIGHEST)
        local_ref[rows, :] = mixed
        start_ref[rows, :] = query * jnp.exp(cum + before)
        before = before + cum[BLOCK - 1 : BLOCK]


def head_kernel(enter_ref, gain_ref, local_ref, start_ref, gate_ref, out_ref):
    mixed = local_ref[...] + nt(start_ref[...], enter_ref[...].astype(F32), precision=HIGHEST)
    scale = lax.rsqrt(jnp.mean(mixed * mixed, axis=-1, keepdims=True) + EPSILON)
    gate = jax.nn.silu(gate_ref[...].astype(F32))
    rows = (mixed * scale * gain_ref[...].astype(F32) * gate).astype(BF16)
    for dest in range(4):
        out_ref[dest] = rows


def project_kernel(ids_ref, heads_ref, w0, w1, w2, w3, out_ref):
    part = ids_ref[0]
    for m in (0, 2):
        pair = ((w0, w1), None, (w2, w3))[m]
        total = jnp.zeros((TOK, 256), F32)
        for h in range(4):
            lanes = slice(h * 128, (h + 1) * 128)
            weight = jnp.concatenate([w[:, lanes] for w in pair], axis=1)
            total = total + jnp.dot(heads_ref[h], weight, preferred_element_type=F32)
        out_ref[part ^ m] = total[:, :128].astype(BF16)
        out_ref[part ^ (m + 1)] = total[:, 128:].astype(BF16)


def places(routing_ref):
    experts = lax.broadcasted_iota(jnp.int32, (TOK, 128), 1)
    hot = [(routing_ref[:, k : k + 1] == experts).astype(F32) for k in range(4)]
    named = hot[0] + hot[1] + hot[2] + hot[3]
    rows = lax.broadcasted_iota(jnp.int32, (TOK, TOK), 0)
    cols = lax.broadcasted_iota(jnp.int32, (TOK, TOK), 1)
    earlier = (rows > cols).astype(BF16)
    ranks = jnp.dot(earlier, named.astype(BF16), preferred_element_type=F32)
    return [
        routing_ref[:, k : k + 1] * MOST
        + jnp.sum(hot[k] * ranks, axis=1, keepdims=True).astype(jnp.int32)
        for k in range(4)
    ]


def pick_kernel(routing_ref, pick_ref):
    place = places(routing_ref)
    slots = lax.broadcasted_iota(jnp.int32, (TOK, 512), 1)
    for j in range(ALL_SLOTS // 512):
        picked = jnp.zeros((TOK, 512), F32)
        for k in range(4):
            picked = picked + (place[k] - j * 512 == slots).astype(F32)
        pick_ref[j * 512 : (j + 1) * 512, :] = picked.T.astype(BF16)


def weigh_kernel(routing_ref, score_ref, high_ref, low_ref):
    place = places(routing_ref)
    scores = [score_ref[:, k : k + 1] for k in range(4)]
    total = scores[0] + scores[1] + scores[2] + scores[3]
    slots = lax.broadcasted_iota(jnp.int32, (TOK, 512), 1)
    for j in range(ALL_SLOTS // 512):
        weighted = jnp.zeros((TOK, 512), F32)
        for k in range(4):
            here = (place[k] - j * 512 == slots).astype(F32)
            weighted = weighted + here * (ROUTE_SCALE * scores[k] / total)
        high = weighted.astype(BF16)
        high_ref[:, j * 512 : (j + 1) * 512] = high
        low_ref[:, j * 512 : (j + 1) * 512] = (weighted - high.astype(F32)).astype(BF16)


def dispatch_kernel(pick_ref, in_ref, residual_ref, out_ref, mid_ref):
    total = residual_ref[...].astype(F32)
    for s in range(4):
        total = total + in_ref[s].astype(F32)
    mid = total.astype(BF16)
    mid_ref[...] = mid
    for j in range(4):
        rows = pl.ds(j * SLOTS, SLOTS)
        picked = jnp.dot(pick_ref[rows, :], mid, preferred_element_type=F32)
        out_ref[rows, :] = picked.astype(BF16)


def expert_kernel(ready, ids_ref, x0, x1, x2, x3, gain_ref, gate_ref, up_ref, out_ref, wide_ref, rows_ref):
    part = ids_ref[0]
    squares = jnp.zeros((SLOTS, 128), F32)
    for m, x_ref in enumerate((x0, x1, x2, x3)):
        for s in range(32):
            wide_ref[m, s * PITCH : s * PITCH + 48, :] = x_ref[s * 48 : (s + 1) * 48, :].astype(F32)
    for m in range(4):
        for q in range(4):
            slab = q * 4 + (part ^ m)
            tile = jnp.concatenate(
                [wide_ref[m, pl.ds(q * MOST + r, 32, stride=PITCH), :] for r in range(MOST)], axis=0
            )
            squares = squares + tile * tile
            scaled = (tile * gain_ref[pl.ds(slab, 1), :]).astype(BF16)
            rows_ref[:, pl.ds(pl.multiple_of(slab * 128, 128), 128)] = scaled
    scale = lax.rsqrt(jnp.sum(squares, axis=1, keepdims=True) * (1.0 / D) + EPSILON)
    ready()
    gate = jnp.dot(rows_ref[...], gate_ref[...], preferred_element_type=F32) * scale
    up = jnp.dot(rows_ref[...], up_ref[...], preferred_element_type=F32) * scale
    out_ref[...] = (jax.nn.silu(gate) * up).astype(BF16)


def down_kernel(h0, h1, h2, h3, d0, d1, d2, d3, out_ref, wide_ref):
    total = jnp.zeros((SLOTS, 512), F32)
    for h_ref, d_ref in ((h0, d0), (h1, d1), (h2, d2), (h3, d3)):
        total = total + jnp.dot(h_ref[...], d_ref[256:512, :], preferred_element_type=F32)
    for q in range(4):
        for r in range(MOST):
            wide_ref[pl.ds(q * MOST + r, 32, stride=PITCH), :] = total[
                r * 32 : (r + 1) * 32, q * 128 : (q + 1) * 128
            ]
    for s in range(32):
        out_ref[s * 48 : (s + 1) * 48, :] = wide_ref[s * PITCH : s * PITCH + 48, :].astype(BF16)


def parts_kernel(ids_ref, project_ref, down_ref, shared_ref, *out_refs):
    part = ids_ref[0]
    for m, out_ref in enumerate(out_refs):
        for q in range(4):
            slab = q * 4 + (part ^ m)
            lanes = slice(q * 128, (q + 1) * 128)
            out_ref[0:256, lanes] = project_ref[pl.ds(pl.multiple_of(slab * 256, 256), 256), :]
            columns = pl.ds(pl.multiple_of(slab * 128, 128), 128)
            out_ref[256:512, lanes] = down_ref[:, columns]
            out_ref[512:576, lanes] = shared_ref[:, columns]


def shared_in_kernel(ids_ref, m0, m1, m2, m3, w0, w1, w2, w3, gain_ref, out_ref, weight_ref, mid_ref):
    part, group = ids_ref[0], ids_ref[1]
    for m, w_ref in enumerate((w0, w1, w2, w3)):
        at = (part ^ m) * 32
        weight_ref[pl.ds(pl.multiple_of(at, 32), 32), :] = w_ref[512:544, :]
        weight_ref[pl.ds(pl.multiple_of(at + 128, 32), 32), :] = w_ref[544:576, :]
    for d, m_ref in enumerate((m0, m1, m2, m3)):
        mid_ref[(group - d) & 3] = m_ref[...]
    squares = jnp.zeros((TOK, 128), F32)
    pre = jnp.zeros((TOK, 256), F32)
    for q in range(4):
        tile = mid_ref[q].astype(F32)
        squares = squares + tile * tile
        scaled = (tile * gain_ref[pl.ds(q * 4 + part, 1), :]).astype(BF16)
        pre = pre + nt(scaled, weight_ref[:, q * 128 : (q + 1) * 128])
    ssq = jnp.sum(squares, axis=1, keepdims=True)
    high = ssq.astype(BF16).astype(F32)
    lane = lax.broadcasted_iota(jnp.int32, (TOK, 128), 1)
    tail = jnp.where(lane == 0, high, jnp.where(lane == 1, ssq - high, 0.0)).astype(BF16)
    out_ref[:, 0:256] = pre.astype(BF16)
    out_ref[:, 256:384] = tail


def shared_hidden_kernel(r0, r1, r2, r3, out_ref):
    total = sum(r[...].astype(F32) for r in (r0, r1, r2, r3))
    ssq = jnp.sum(total[:, 256:384], axis=1, keepdims=True)
    scale = lax.rsqrt(ssq * (1.0 / D) + EPSILON)
    hidden = jax.nn.silu(total[:, 0:128] * scale) * (total[:, 128:256] * scale)
    out_ref[...] = hidden.astype(BF16)


def final_kernel(ids_ref, back_ref, high_ref, low_ref, h0, h1, h2, h3, down_ref, mid_ref, out_ref):
    group = ids_ref[1]
    back = back_ref[...]
    total = mid_ref[...].astype(F32)
    total = total + jnp.dot(high_ref[...], back, preferred_element_type=F32)
    total = total + jnp.dot(low_ref[...], back, preferred_element_type=F32)
    for d, h in enumerate((h0, h1, h2, h3)):
        at = pl.multiple_of(((group - d) & 3) * 128, 128)
        total = total + jnp.dot(
            h[...], down_ref[pl.ds(at, 128), :], preferred_element_type=F32
        )
    out_ref[...] = total.astype(BF16)


def exchange(value, axes):
    return lax.all_to_all(value, axes, split_axis=0, concat_axis=0, tiled=True)


def moved(value, axes, target):
    count = lax.axis_size(axes)
    return lax.ppermute(value, axes, [(i, target(i) % count) for i in range(count)])


def shifted(values, axes):
    return [moved(v, axes, lambda i, d=d: i + d) for d, v in enumerate(values, 1)]


def swapped(value, axis):
    return moved(value, axis, lambda i: i ^ 1)


def grouped(values):
    return [moved(v, GROUP, lambda i, m=m: i ^ m) for m, v in enumerate(values, 1)]


def body(
    queries,
    key_matrix,
    value_matrix,
    output_gate_preactivation,
    decay_preactivation,
    extra_log_decay,
    head_norm_gain,
    output_projection,
    residual,
    feedforward_gain,
    routing,
    router_score,
    expert_gate_weight,
    expert_up_weight,
    expert_down_weight,
    shared_expert_gate,
    shared_expert_up,
    shared_expert_down,
):
    ids = jnp.stack([lax.axis_index(a) for a in (GROUP, "yg")]).astype(jnp.int32)
    gain = feedforward_gain.astype(F32).reshape(16, 128)
    head_gain = head_norm_gain.reshape(1, DV)
    extra = extra_log_decay.reshape(2, 128)
    whole = (0, TOK)

    payload = call(
        state_kernel, ((32, 16, DK), BF16),
        key_matrix, value_matrix, decay_preactivation, extra, fetch=(whole, whole, whole, (0, 2)), limit=60,
    )
    states = exchange(payload, SP)
    local, start = call(
        local_kernel, [((TOK, DV), F32), ((TOK, DK), F32)],
        queries, key_matrix, value_matrix, decay_preactivation, extra,
        fetch=(whole, whole, whole, whole, (0, 2)), limit=60,
    )
    pick = call(pick_kernel, ((ALL_SLOTS, TOK), BF16), routing)
    high, low = call(
        weigh_kernel, [((TOK, ALL_SLOTS), BF16), ((TOK, ALL_SLOTS), BF16)], routing, router_score
    )
    shared_in = jnp.concatenate([shared_expert_gate.T, shared_expert_up.T], axis=0)
    own_part, *far_parts = call(
        parts_kernel, [((576, 512), BF16)] * 4,
        ids, output_projection, expert_down_weight, shared_in, smem=1,
    )
    parts = [own_part] + grouped(far_parts)

    entering = exchange(call(scan_kernel, ((32, 8, DK), BF16), states), SP)
    head_rows = call(
        head_kernel, ((4, TOK, DV), BF16),
        entering.reshape(DV, DK), head_gain, local, start, output_gate_preactivation,
        fetch=(whole, whole, whole),
    )
    partial = call(
        project_kernel, ((4, TOK, 128), BF16),
        ids, exchange(head_rows, "yg"), *parts, smem=1, fetch=(whole,) * 4,
    )
    outgoing, mid = call(
        dispatch_kernel, [((ALL_SLOTS, 128), BF16), ((TOK, 128), BF16)],
        pick, exchange(partial, GROUP), residual,
    )
    own = exchange(outgoing.reshape(128, 3, 4, 128), SPG).reshape(ALL_SLOTS, 128)
    mids = [mid] + shifted([mid] * 3, "yg")

    across = swapped(own, "yn")
    beside = swapped(own, "c")
    far = swapped(across, "c")
    pre = call(
        shared_in_kernel, ((TOK, 384), BF16), ids, *mids, *parts, gain, smem=1,
        scratch=[pltpu.VMEM((256, 512), BF16), pltpu.VMEM((4, TOK, 128), BF16)],
    )
    pre = [pre] + grouped([pre] * 3)
    routed = call(
        expert_kernel, ((SLOTS, 256), BF16),
        ids, own, beside, across, far, gain, expert_gate_weight, expert_up_weight,
        smem=1, fetch=((0, D), (0, D)), late=True,
        scratch=[pltpu.VMEM((4, 32 * PITCH, 128), F32), pltpu.VMEM((SLOTS, D), BF16)],
    )
    routed_across = swapped(routed, "yn")
    routed_beside = swapped(routed, "c")
    routed_far = swapped(routed_across, "c")
    expert_out = call(
        down_kernel, ((ALL_SLOTS, 128), BF16),
        routed, routed_beside, routed_across, routed_far, *parts,
        scratch=[pltpu.VMEM((32 * PITCH, 128), F32)],
    )
    back = exchange(expert_out.reshape(128, 3, 4, 128), SPG).reshape(ALL_SLOTS, 128)
    hidden = call(shared_hidden_kernel, ((TOK, 128), BF16), *pre)
    hidden = [hidden] + shifted([hidden] * 3, "yg")
    return call(
        final_kernel, ((TOK, 128), BF16),
        ids, back, high, low, *hidden, shared_expert_down, mid, smem=1,
    )


def solution(mesh):
    finer = Mesh(mesh.devices.reshape(8, 4, 4, 2, 2), ("z", "x", "yg", "yn", "c"))
    in_specs = (
        P(SP, TP),
        P(SP, TP),
        P(SP, TP),
        P(SP, TP),
        P(SP, TP),
        P(SP, TP),
        P(),
        P(None, TP),
        P(SP, TP),
        P(),
        P(SP, None),
        P(SP, None),
        P(None, SP + TP),
        P(None, SP + TP),
        P(SP + TP, None),
        P(None, TP),
        P(None, TP),
        P(None, TP),
    )
    return jax.shard_map(body, mesh=finer, in_specs=in_specs, out_specs=P(SP, TP), check_vma=False)
```

```python
import jax
import jax.numpy as jnp
from jax import lax
from jax.experimental import pallas as pl
from jax.experimental.pallas import tpu as pltpu
from jax.sharding import Mesh
from jax.sharding import PartitionSpec as P

DK = 128
DV = 256
BLOCK = 64
TOK = 256
MOST = 12
SLOTS = 384
ALL_SLOTS = 1536
PITCH = 56
D = 2048
SP = ("z", "x")
SPG = ("z", "x", "yg")
TP = ("yg", "yn", "c")
GROUP = ("yn", "c")
F32 = jnp.float32
BF16 = jnp.bfloat16
HIGHEST = lax.Precision.HIGHEST
EPSILON = 1e-06
ROUTE_SCALE = 2.5
GATE_TEMPER = 16.0
VMEM = pl.BlockSpec(memory_space=pltpu.VMEM)
SMEM = pl.BlockSpec(memory_space=pltpu.SMEM)


def call(kernel, outs, *args, scratch=(), smem=0, fetch=(), late=False, limit=24):
    single = not isinstance(outs, list)
    shapes = [jax.ShapeDtypeStruct(s, t) for s, t in ([outs] if single else outs)]
    n_in, n_out, n_scratch, n_fetch = len(args), len(shapes), len(scratch), len(fetch)
    kept = n_in - n_fetch
    buffers = []
    for arg, rows in zip(args[kept:], fetch, strict=True):
        buffers.append(pltpu.VMEM((rows[1], *arg.shape[1:]), arg.dtype))

    def fetching(*refs):
        sources, results = refs[kept:n_in], refs[n_in : n_in + n_out]
        own = refs[n_in + n_out : n_in + n_out + n_scratch]
        held, sems = refs[n_in + n_out + n_scratch : -1], refs[-1]
        copies = [
            pltpu.make_async_copy(src.at[pl.ds(rows[0], rows[1])], dst, sems.at[i])
            for i, (src, dst, rows) in enumerate(zip(sources, held, fetch, strict=True))
        ]
        for copy in copies:
            copy.start()

        def ready():
            for copy in copies:
                copy.wait()

        if late:
            kernel(ready, *refs[:kept], *held, *results, *own)
        else:
            ready()
            kernel(*refs[:kept], *held, *results, *own)

    extra = buffers + [pltpu.SemaphoreType.DMA((n_fetch,))] if fetch else []
    any_spec = pl.BlockSpec(memory_space=pl.ANY)
    got = pl.pallas_call(
        fetching if fetch else kernel,
        out_shape=shapes,
        in_specs=[SMEM] * smem + [VMEM] * (kept - smem) + [any_spec] * n_fetch,
        out_specs=[VMEM] * n_out,
        scratch_shapes=list(scratch) + extra,
        compiler_params=pltpu.CompilerParams(vmem_limit_bytes=limit * 2**20),
        cost_estimate=pl.CostEstimate(
            flops=1000000, bytes_accessed=1000000, transcendentals=0
        ),
    )(*args)
    return got[0] if single else got


def nt(a, b, **kw):
    return lax.dot_general(
        a, b, (((1,), (1,)), ((), ())), preferred_element_type=F32, **kw
    )


def decays(decay_ref, extra_ref):
    raw = decay_ref[...].astype(F32)
    logs = jax.nn.log_sigmoid(raw) / GATE_TEMPER
    rows = lax.broadcasted_iota(jnp.int32, (BLOCK, BLOCK), 0)
    cols = lax.broadcasted_iota(jnp.int32, (BLOCK, BLOCK), 1)
    lower = (rows >= cols).astype(F32)
    wide_rows = lax.broadcasted_iota(jnp.int32, (BLOCK, 128), 0)
    wide_cols = lax.broadcasted_iota(jnp.int32, (BLOCK, 128), 1)
    ones = jnp.ones((128, DK), F32)
    inside = []
    for b in range(TOK // BLOCK):
        at = wide_cols - (b % 2) * BLOCK
        extra = jnp.where((at >= 0) & (at <= wide_rows), extra_ref[b // 2 : b // 2 + 1, :], 0.0)
        inside.append(
            jnp.dot(lower, logs[b * BLOCK : (b + 1) * BLOCK], precision=HIGHEST,
                    preferred_element_type=F32)
            + jnp.dot(extra, ones, precision=HIGHEST, preferred_element_type=F32)
        )
    return inside


def block_states(inside, key_ref, value_ref):
    state = jnp.zeros((DV, DK), F32)
    states = []
    total = jnp.zeros((1, DK), F32)
    for b, cum in enumerate(inside):
        states.append(state)
        rows = pl.ds(b * BLOCK, BLOCK)
        end = cum[BLOCK - 1 : BLOCK]
        key_end = key_ref[rows, :].astype(F32) * jnp.exp(end - cum)
        value = value_ref[rows, :].astype(F32)
        fresh = jnp.dot(value.T, key_end, precision=HIGHEST, preferred_element_type=F32)
        state = jnp.exp(end) * state + fresh
        total = total + end
    return states, state, total


def state_kernel(key_ref, value_ref, decay_ref, extra_ref, out_ref):
    inside = decays(decay_ref, extra_ref)
    _, state, total = block_states(inside, key_ref, value_ref)
    out_ref[:, 0:8, :] = state.reshape(32, 8, DK).astype(BF16)
    decay = jnp.exp(total)
    high = decay.astype(BF16).astype(F32)
    row = lax.broadcasted_iota(jnp.int32, (8, DK), 0)
    tail = jnp.where(row == 0, high, jnp.where(row == 1, decay - high, 0.0))
    out_ref[:, 8:16, :] = jnp.broadcast_to(tail[None], (32, 8, DK)).astype(BF16)


def scan_kernel(in_ref, out_ref):
    state = jnp.zeros((8, DK), F32)
    for s in range(32):
        out_ref[s] = state.astype(BF16)
        block = in_ref[s].astype(F32)
        decay = block[8:9] + block[9:10]
        state = decay * state + block[0:8]


def local_kernel(query_ref, key_ref, value_ref, decay_ref, extra_ref, local_ref, start_ref):
    inside = decays(decay_ref, extra_ref)
    states, _, _ = block_states(inside, key_ref, value_ref)
    rows_at = lax.broadcasted_iota(jnp.int32, (BLOCK, BLOCK), 0)
    cols_at = lax.broadcasted_iota(jnp.int32, (BLOCK, BLOCK), 1)
    before = jnp.zeros((1, DK), F32)
    for b, cum in enumerate(inside):
        rows = pl.ds(b * BLOCK, BLOCK)
        query = query_ref[rows, :].astype(F32) * DK ** (-0.5)
        key = key_ref[rows, :].astype(F32)
        value = value_ref[rows, :].astype(F32)
        query_decay = query * jnp.exp(cum)
        scores = nt(query_decay, key * jnp.exp(-cum), precision=HIGHEST)
        scores = jnp.where(rows_at >= cols_at, scores, 0.0)
        mixed = jnp.dot(scores, value, precision=HIGHEST, preferred_element_type=F32)
        if b > 0:
            mixed = mixed + nt(query_decay, states[b], precision=HIGHEST)
        local_ref[rows, :] = mixed
        start_ref[rows, :] = query * jnp.exp(cum + before)
        before = before + cum[BLOCK - 1 : BLOCK]


def head_kernel(gain_ref, enter_ref, local_ref, start_ref, gate_ref, out_ref):
    mixed = local_ref[...] + nt(start_ref[...], enter_ref[...].astype(F32), precision=HIGHEST)
    scale = lax.rsqrt(jnp.mean(mixed * mixed, axis=-1, keepdims=True) + EPSILON)
    gate = jax.nn.silu(gate_ref[...].astype(F32))
    rows = (mixed * scale * gain_ref[...].astype(F32) * gate).astype(BF16)
    for dest in range(4):
        out_ref[dest] = rows


def project_kernel(ids_ref, heads_ref, w0, w1, w2, w3, out_ref):
    part = ids_ref[0]
    for m in (0, 2):
        pair = ((w0, w1), None, (w2, w3))[m]
        total = jnp.zeros((TOK, 256), F32)
        for h in range(4):
            lanes = slice(h * 128, (h + 1) * 128)
            weight = jnp.concatenate([w[:, lanes] for w in pair], axis=1)
            total = total + jnp.dot(heads_ref[h], weight, preferred_element_type=F32)
        out_ref[part ^ m] = total[:, :128].astype(BF16)
        out_ref[part ^ (m + 1)] = total[:, 128:].astype(BF16)


def places(routing_ref):
    experts = lax.broadcasted_iota(jnp.int32, (TOK, 128), 1)
    hot = [(routing_ref[:, k : k + 1] == experts).astype(F32) for k in range(4)]
    named = hot[0] + hot[1] + hot[2] + hot[3]
    rows = lax.broadcasted_iota(jnp.int32, (TOK, TOK), 0)
    cols = lax.broadcasted_iota(jnp.int32, (TOK, TOK), 1)
    earlier = (rows > cols).astype(BF16)
    ranks = jnp.dot(earlier, named.astype(BF16), preferred_element_type=F32)
    return [
        routing_ref[:, k : k + 1] * MOST
        + jnp.sum(hot[k] * ranks, axis=1, keepdims=True).astype(jnp.int32)
        for k in range(4)
    ]


def pick_kernel(routing_ref, pick_ref):
    place = places(routing_ref)
    slots = lax.broadcasted_iota(jnp.int32, (TOK, 512), 1)
    for j in range(ALL_SLOTS // 512):
        picked = jnp.zeros((TOK, 512), F32)
        for k in range(4):
            picked = picked + (place[k] - j * 512 == slots).astype(F32)
        pick_ref[j * 512 : (j + 1) * 512, :] = picked.T.astype(BF16)


def weigh_kernel(routing_ref, score_ref, high_ref, low_ref):
    place = places(routing_ref)
    scores = [score_ref[:, k : k + 1] for k in range(4)]
    total = scores[0] + scores[1] + scores[2] + scores[3]
    slots = lax.broadcasted_iota(jnp.int32, (TOK, 512), 1)
    for j in range(ALL_SLOTS // 512):
        weighted = jnp.zeros((TOK, 512), F32)
        for k in range(4):
            here = (place[k] - j * 512 == slots).astype(F32)
            weighted = weighted + here * (ROUTE_SCALE * scores[k] / total)
        high = weighted.astype(BF16)
        high_ref[:, j * 512 : (j + 1) * 512] = high
        low_ref[:, j * 512 : (j + 1) * 512] = (weighted - high.astype(F32)).astype(BF16)


def dispatch_kernel(pick_ref, in_ref, residual_ref, out_ref, mid_ref):
    total = residual_ref[...].astype(F32)
    for s in range(4):
        total = total + in_ref[s].astype(F32)
    mid = total.astype(BF16)
    mid_ref[...] = mid
    for j in range(4):
        rows = pl.ds(j * SLOTS, SLOTS)
        picked = jnp.dot(pick_ref[rows, :], mid, preferred_element_type=F32)
        out_ref[rows, :] = picked.astype(BF16)


def expert_kernel(ready, ids_ref, x0, x1, x2, x3, gain_ref, gate_ref, up_ref, out_ref, wide_ref, rows_ref):
    part = ids_ref[0]
    squares = jnp.zeros((SLOTS, 128), F32)
    for m, x_ref in enumerate((x0, x1, x2, x3)):
        for s in range(32):
            wide_ref[m, s * PITCH : s * PITCH + 48, :] = x_ref[s * 48 : (s + 1) * 48, :].astype(F32)
    for m in range(4):
        for q in range(4):
            slab = q * 4 + (part ^ m)
            tile = jnp.concatenate(
                [wide_ref[m, pl.ds(q * MOST + r, 32, stride=PITCH), :] for r in range(MOST)], axis=0
            )
            squares = squares + tile * tile
            scaled = (tile * gain_ref[pl.ds(slab, 1), :]).astype(BF16)
            rows_ref[:, pl.ds(pl.multiple_of(slab * 128, 128), 128)] = scaled
    scale = lax.rsqrt(jnp.sum(squares, axis=1, keepdims=True) * (1.0 / D) + EPSILON)
    ready()
    gate = jnp.dot(rows_ref[...], gate_ref[...], preferred_element_type=F32) * scale
    up = jnp.dot(rows_ref[...], up_ref[...], preferred_element_type=F32) * scale
    out_ref[...] = (jax.nn.silu(gate) * up).astype(BF16)


def gain_kernel(in_ref, out_ref):
    out_ref[...] = in_ref[...].astype(F32)


def down_kernel(h0, h1, h2, h3, d0, d1, d2, d3, out_ref, wide_ref):
    total = jnp.zeros((SLOTS, 512), F32)
    for h_ref, d_ref in ((h0, d0), (h1, d1), (h2, d2), (h3, d3)):
        total = total + jnp.dot(h_ref[...], d_ref[256:512, :], preferred_element_type=F32)
    for q in range(4):
        for r in range(MOST):
            wide_ref[pl.ds(q * MOST + r, 32, stride=PITCH), :] = total[
                r * 32 : (r + 1) * 32, q * 128 : (q + 1) * 128
            ]
    for s in range(32):
        out_ref[s * 48 : (s + 1) * 48, :] = wide_ref[s * PITCH : s * PITCH + 48, :].astype(BF16)


def parts_kernel(ids_ref, project_ref, down_ref, shared_ref, *out_refs):
    part = ids_ref[0]
    for m, out_ref in enumerate(out_refs):
        for q in range(4):
            slab = q * 4 + (part ^ m)
            lanes = slice(q * 128, (q + 1) * 128)
            out_ref[0:256, lanes] = project_ref[pl.ds(pl.multiple_of(slab * 256, 256), 256), :]
            columns = pl.ds(pl.multiple_of(slab * 128, 128), 128)
            out_ref[256:512, lanes] = down_ref[:, columns]
            out_ref[512:576, lanes] = shared_ref[:, columns]


def shared_in_kernel(ids_ref, m0, m1, m2, m3, w0, w1, w2, w3, gain_ref, out_ref, weight_ref, mid_ref):
    part, group = ids_ref[0], ids_ref[1]
    for m, w_ref in enumerate((w0, w1, w2, w3)):
        at = (part ^ m) * 32
        weight_ref[pl.ds(pl.multiple_of(at, 32), 32), :] = w_ref[512:544, :]
        weight_ref[pl.ds(pl.multiple_of(at + 128, 32), 32), :] = w_ref[544:576, :]
    for d, m_ref in enumerate((m0, m1, m2, m3)):
        mid_ref[(group - d) & 3] = m_ref[...]
    squares = jnp.zeros((TOK, 128), F32)
    pre = jnp.zeros((TOK, 256), F32)
    for q in range(4):
        tile = mid_ref[q].astype(F32)
        squares = squares + tile * tile
        scaled = (tile * gain_ref[pl.ds(q * 4 + part, 1), :]).astype(BF16)
        pre = pre + nt(scaled, weight_ref[:, q * 128 : (q + 1) * 128])
    ssq = jnp.sum(squares, axis=1, keepdims=True)
    high = ssq.astype(BF16).astype(F32)
    lane = lax.broadcasted_iota(jnp.int32, (TOK, 128), 1)
    tail = jnp.where(lane == 0, high, jnp.where(lane == 1, ssq - high, 0.0)).astype(BF16)
    out_ref[:, 0:256] = pre.astype(BF16)
    out_ref[:, 256:384] = tail


def shared_hidden_kernel(r0, r1, r2, r3, out_ref):
    total = sum(r[...].astype(F32) for r in (r0, r1, r2, r3))
    ssq = jnp.sum(total[:, 256:384], axis=1, keepdims=True)
    scale = lax.rsqrt(ssq * (1.0 / D) + EPSILON)
    hidden = jax.nn.silu(total[:, 0:128] * scale) * (total[:, 128:256] * scale)
    out_ref[...] = hidden.astype(BF16)


def ahead_kernel(ids_ref, h0, h1, h2, h3, down_ref, mid_ref, out_ref):
    group = ids_ref[1]
    total = mid_ref[...].astype(F32)
    for d, h in enumerate((h0, h1, h2, h3)):
        at = pl.multiple_of(((group - d) & 3) * 128, 128)
        total = total + jnp.dot(
            h[...], down_ref[pl.ds(at, 128), :], preferred_element_type=F32
        )
    out_ref[...] = total


def final_kernel(back_ref, high_ref, low_ref, ahead_ref, out_ref):
    back = back_ref[...]
    total = ahead_ref[...] + jnp.dot(high_ref[...], back, preferred_element_type=F32)
    total = total + jnp.dot(low_ref[...], back, preferred_element_type=F32)
    out_ref[...] = total.astype(BF16)


def exchange(value, axes):
    return lax.all_to_all(value, axes, split_axis=0, concat_axis=0, tiled=True)


def moved(value, axes, target):
    count = lax.axis_size(axes)
    return lax.ppermute(value, axes, [(i, target(i) % count) for i in range(count)])


def shifted(values, axes):
    return [moved(v, axes, lambda i, d=d: i + d) for d, v in enumerate(values, 1)]


def swapped(value, axis):
    return moved(value, axis, lambda i: i ^ 1)


def grouped(values):
    return [moved(v, GROUP, lambda i, m=m: i ^ m) for m, v in enumerate(values, 1)]


def body(
    queries,
    key_matrix,
    value_matrix,
    output_gate_preactivation,
    decay_preactivation,
    extra_log_decay,
    head_norm_gain,
    output_projection,
    residual,
    feedforward_gain,
    routing,
    router_score,
    expert_gate_weight,
    expert_up_weight,
    expert_down_weight,
    shared_expert_gate,
    shared_expert_up,
    shared_expert_down,
):
    ids = jnp.stack([lax.axis_index(a) for a in (GROUP, "yg")]).astype(jnp.int32)
    gain = call(gain_kernel, ((16, 128), F32), feedforward_gain.reshape(16, 128))
    head_gain = head_norm_gain.reshape(1, DV)
    extra = extra_log_decay.reshape(2, 128)
    whole = (0, TOK)

    payload = call(
        state_kernel, ((32, 16, DK), BF16),
        key_matrix, value_matrix, decay_preactivation, extra, fetch=(whole, whole, whole, (0, 2)), limit=60,
    )
    states = exchange(payload, SP)
    local, start = call(
        local_kernel, [((TOK, DV), F32), ((TOK, DK), F32)],
        queries, key_matrix, value_matrix, decay_preactivation, extra,
        fetch=(whole, whole, whole, whole, (0, 2)), limit=60,
    )
    pick = call(pick_kernel, ((ALL_SLOTS, TOK), BF16), routing)
    high, low = call(
        weigh_kernel, [((TOK, ALL_SLOTS), BF16), ((TOK, ALL_SLOTS), BF16)], routing, router_score
    )
    shared_in = jnp.concatenate([shared_expert_gate.T, shared_expert_up.T], axis=0)
    own_part, *far_parts = call(
        parts_kernel, [((576, 512), BF16)] * 4,
        ids, output_projection, expert_down_weight, shared_in, smem=1,
    )
    parts = [own_part] + grouped(far_parts)

    entering = exchange(call(scan_kernel, ((32, 8, DK), BF16), states), SP)
    head_rows = call(
        head_kernel, ((4, TOK, DV), BF16),
        head_gain, entering.reshape(DV, DK), local, start, output_gate_preactivation,
        fetch=(whole,) * 4, limit=60,
    )
    partial = call(
        project_kernel, ((4, TOK, 128), BF16),
        ids, exchange(head_rows, "yg"), *parts, smem=1, fetch=(whole,) * 4,
    )
    outgoing, mid = call(
        dispatch_kernel, [((ALL_SLOTS, 128), BF16), ((TOK, 128), BF16)],
        pick, exchange(partial, GROUP), residual,
    )
    own = exchange(outgoing.reshape(128, 3, 4, 128), SPG).reshape(ALL_SLOTS, 128)
    mids = [mid] + shifted([mid] * 3, "yg")

    across = swapped(own, "yn")
    beside = swapped(own, "c")
    far = swapped(across, "c")
    pre = call(
        shared_in_kernel, ((TOK, 384), BF16), ids, *mids, *parts, gain, smem=1,
        scratch=[pltpu.VMEM((256, 512), BF16), pltpu.VMEM((4, TOK, 128), BF16)],
    )
    pre = [pre] + grouped([pre] * 3)
    routed = call(
        expert_kernel, ((SLOTS, 256), BF16),
        ids, own, beside, across, far, gain, expert_gate_weight, expert_up_weight,
        smem=1, fetch=((0, D), (0, D)), late=True,
        scratch=[pltpu.VMEM((4, 32 * PITCH, 128), F32), pltpu.VMEM((SLOTS, D), BF16)],
    )
    routed_across = swapped(routed, "yn")
    routed_beside = swapped(routed, "c")
    routed_far = swapped(routed_across, "c")
    expert_out = call(
        down_kernel, ((ALL_SLOTS, 128), BF16),
        routed, routed_beside, routed_across, routed_far, *parts,
        scratch=[pltpu.VMEM((32 * PITCH, 128), F32)],
    )
    back = exchange(expert_out.reshape(128, 3, 4, 128), SPG).reshape(ALL_SLOTS, 128)
    hidden = call(shared_hidden_kernel, ((TOK, 128), BF16), *pre)
    hidden = [hidden] + shifted([hidden] * 3, "yg")
    ahead = call(
        ahead_kernel, ((TOK, 128), F32), ids, *hidden, shared_expert_down, mid, smem=1,
    )
    return call(final_kernel, ((TOK, 128), BF16), back, high, low, ahead)


def solution(mesh):
    finer = Mesh(mesh.devices.reshape(8, 4, 4, 2, 2), ("z", "x", "yg", "yn", "c"))
    in_specs = (
        P(SP, TP),
        P(SP, TP),
        P(SP, TP),
        P(SP, TP),
        P(SP, TP),
        P(SP, TP),
        P(),
        P(None, TP),
        P(SP, TP),
        P(),
        P(SP, None),
        P(SP, None),
        P(None, SP + TP),
        P(None, SP + TP),
        P(SP + TP, None),
        P(None, TP),
        P(None, TP),
        P(None, TP),
    )
    return jax.shard_map(body, mesh=finer, in_specs=in_specs, out_specs=P(SP, TP), check_vma=False)
```

```python
import jax
import jax.numpy as jnp
from jax import lax
from jax.experimental import pallas as pl
from jax.experimental.pallas import tpu as pltpu
from jax.sharding import Mesh
from jax.sharding import PartitionSpec as P

DK = 128
DV = 256
BLOCK = 64
TOK = 256
MOST = 12
SLOTS = 384
ALL_SLOTS = 1536
PITCH = 56
D = 2048
SP = ("z", "x")
SPG = ("z", "x", "yg")
TP = ("yg", "yn", "c")
GROUP = ("yn", "c")
F32 = jnp.float32
BF16 = jnp.bfloat16
HIGHEST = lax.Precision.HIGHEST
EPSILON = 1e-06
ROUTE_SCALE = 2.5
GATE_TEMPER = 16.0
VMEM = pl.BlockSpec(memory_space=pltpu.VMEM)
SMEM = pl.BlockSpec(memory_space=pltpu.SMEM)


def call(kernel, outs, *args, scratch=(), smem=0, fetch=(), late=False, limit=24):
    single = not isinstance(outs, list)
    shapes = [jax.ShapeDtypeStruct(s, t) for s, t in ([outs] if single else outs)]
    n_in, n_out, n_scratch, n_fetch = len(args), len(shapes), len(scratch), len(fetch)
    kept = n_in - n_fetch
    buffers = []
    for arg, rows in zip(args[kept:], fetch, strict=True):
        buffers.append(pltpu.VMEM((rows[1], *arg.shape[1:]), arg.dtype))

    def fetching(*refs):
        sources, results = refs[kept:n_in], refs[n_in : n_in + n_out]
        own = refs[n_in + n_out : n_in + n_out + n_scratch]
        held, sems = refs[n_in + n_out + n_scratch : -1], refs[-1]
        copies = [
            pltpu.make_async_copy(src.at[pl.ds(rows[0], rows[1])], dst, sems.at[i])
            for i, (src, dst, rows) in enumerate(zip(sources, held, fetch, strict=True))
        ]
        for copy in copies:
            copy.start()

        def ready():
            for copy in copies:
                copy.wait()

        if late:
            kernel(ready, *refs[:kept], *held, *results, *own)
        else:
            ready()
            kernel(*refs[:kept], *held, *results, *own)

    extra = buffers + [pltpu.SemaphoreType.DMA((n_fetch,))] if fetch else []
    any_spec = pl.BlockSpec(memory_space=pl.ANY)
    got = pl.pallas_call(
        fetching if fetch else kernel,
        out_shape=shapes,
        in_specs=[SMEM] * smem + [VMEM] * (kept - smem) + [any_spec] * n_fetch,
        out_specs=[VMEM] * n_out,
        scratch_shapes=list(scratch) + extra,
        compiler_params=pltpu.CompilerParams(vmem_limit_bytes=limit * 2**20),
        cost_estimate=pl.CostEstimate(
            flops=1000000, bytes_accessed=1000000, transcendentals=0
        ),
    )(*args)
    return got[0] if single else got


def nt(a, b, **kw):
    return lax.dot_general(
        a, b, (((1,), (1,)), ((), ())), preferred_element_type=F32, **kw
    )


def decays(decay_ref, extra_ref):
    raw = decay_ref[...].astype(F32)
    logs = jax.nn.log_sigmoid(raw) / GATE_TEMPER
    rows = lax.broadcasted_iota(jnp.int32, (BLOCK, BLOCK), 0)
    cols = lax.broadcasted_iota(jnp.int32, (BLOCK, BLOCK), 1)
    lower = (rows >= cols).astype(F32)
    wide_rows = lax.broadcasted_iota(jnp.int32, (BLOCK, 128), 0)
    wide_cols = lax.broadcasted_iota(jnp.int32, (BLOCK, 128), 1)
    ones = jnp.ones((128, DK), F32)
    inside = []
    for b in range(TOK // BLOCK):
        at = wide_cols - (b % 2) * BLOCK
        extra = jnp.where((at >= 0) & (at <= wide_rows), extra_ref[b // 2 : b // 2 + 1, :], 0.0)
        inside.append(
            jnp.dot(lower, logs[b * BLOCK : (b + 1) * BLOCK], precision=HIGHEST,
                    preferred_element_type=F32)
            + jnp.dot(extra, ones, precision=HIGHEST, preferred_element_type=F32)
        )
    return inside


def block_states(inside, key_ref, value_ref):
    state = jnp.zeros((DV, DK), F32)
    states = []
    total = jnp.zeros((1, DK), F32)
    for b, cum in enumerate(inside):
        states.append(state)
        rows = pl.ds(b * BLOCK, BLOCK)
        end = cum[BLOCK - 1 : BLOCK]
        key_end = key_ref[rows, :].astype(F32) * jnp.exp(end - cum)
        value = value_ref[rows, :].astype(F32)
        fresh = jnp.dot(value.T, key_end, precision=HIGHEST, preferred_element_type=F32)
        state = jnp.exp(end) * state + fresh
        total = total + end
    return states, state, total


def state_kernel(key_ref, value_ref, decay_ref, extra_ref, out_ref):
    inside = decays(decay_ref, extra_ref)
    _, state, total = block_states(inside, key_ref, value_ref)
    out_ref[:, 0:8, :] = state.reshape(32, 8, DK).astype(BF16)
    decay = jnp.exp(total)
    high = decay.astype(BF16).astype(F32)
    row = lax.broadcasted_iota(jnp.int32, (8, DK), 0)
    tail = jnp.where(row == 0, high, jnp.where(row == 1, decay - high, 0.0))
    out_ref[:, 8:16, :] = jnp.broadcast_to(tail[None], (32, 8, DK)).astype(BF16)


def scan_kernel(in_ref, out_ref):
    state = jnp.zeros((8, DK), F32)
    for s in range(32):
        out_ref[s] = state.astype(BF16)
        block = in_ref[s].astype(F32)
        decay = block[8:9] + block[9:10]
        state = decay * state + block[0:8]


def local_kernel(query_ref, key_ref, value_ref, decay_ref, extra_ref, local_ref, start_ref):
    inside = decays(decay_ref, extra_ref)
    states, _, _ = block_states(inside, key_ref, value_ref)
    rows_at = lax.broadcasted_iota(jnp.int32, (BLOCK, BLOCK), 0)
    cols_at = lax.broadcasted_iota(jnp.int32, (BLOCK, BLOCK), 1)
    before = jnp.zeros((1, DK), F32)
    for b, cum in enumerate(inside):
        rows = pl.ds(b * BLOCK, BLOCK)
        query = query_ref[rows, :].astype(F32) * DK ** (-0.5)
        key = key_ref[rows, :].astype(F32)
        value = value_ref[rows, :].astype(F32)
        query_decay = query * jnp.exp(cum)
        scores = nt(query_decay, key * jnp.exp(-cum), precision=HIGHEST)
        scores = jnp.where(rows_at >= cols_at, scores, 0.0)
        mixed = jnp.dot(scores, value, precision=HIGHEST, preferred_element_type=F32)
        if b > 0:
            mixed = mixed + nt(query_decay, states[b], precision=HIGHEST)
        local_ref[rows, :] = mixed
        start_ref[rows, :] = query * jnp.exp(cum + before)
        before = before + cum[BLOCK - 1 : BLOCK]


def head_kernel(enter_ref, gain_ref, local_ref, start_ref, gate_ref, out_ref):
    mixed = local_ref[...] + nt(start_ref[...], enter_ref[...].astype(F32), precision=HIGHEST)
    scale = lax.rsqrt(jnp.mean(mixed * mixed, axis=-1, keepdims=True) + EPSILON)
    gate = jax.nn.silu(gate_ref[...].astype(F32))
    rows = (mixed * scale * gain_ref[...].astype(F32) * gate).astype(BF16)
    for dest in range(4):
        out_ref[dest] = rows


def project_kernel(ids_ref, heads_ref, w0, w1, w2, w3, out_ref):
    part = ids_ref[0]
    for m in (0, 2):
        pair = ((w0, w1), None, (w2, w3))[m]
        total = jnp.zeros((TOK, 256), F32)
        for h in range(4):
            lanes = slice(h * 128, (h + 1) * 128)
            weight = jnp.concatenate([w[:, lanes] for w in pair], axis=1)
            total = total + jnp.dot(heads_ref[h], weight, preferred_element_type=F32)
        out_ref[part ^ m] = total[:, :128].astype(BF16)
        out_ref[part ^ (m + 1)] = total[:, 128:].astype(BF16)


def places(routing_ref):
    experts = lax.broadcasted_iota(jnp.int32, (TOK, 128), 1)
    hot = [(routing_ref[:, k : k + 1] == experts).astype(F32) for k in range(4)]
    named = hot[0] + hot[1] + hot[2] + hot[3]
    rows = lax.broadcasted_iota(jnp.int32, (TOK, TOK), 0)
    cols = lax.broadcasted_iota(jnp.int32, (TOK, TOK), 1)
    earlier = (rows > cols).astype(BF16)
    ranks = jnp.dot(earlier, named.astype(BF16), preferred_element_type=F32)
    return [
        routing_ref[:, k : k + 1] * MOST
        + jnp.sum(hot[k] * ranks, axis=1, keepdims=True).astype(jnp.int32)
        for k in range(4)
    ]


def pick_kernel(routing_ref, pick_ref):
    place = places(routing_ref)
    slots = lax.broadcasted_iota(jnp.int32, (TOK, 512), 1)
    for j in range(ALL_SLOTS // 512):
        picked = jnp.zeros((TOK, 512), F32)
        for k in range(4):
            picked = picked + (place[k] - j * 512 == slots).astype(F32)
        pick_ref[j * 512 : (j + 1) * 512, :] = picked.T.astype(BF16)


def weigh_kernel(routing_ref, score_ref, high_ref, low_ref):
    place = places(routing_ref)
    scores = [score_ref[:, k : k + 1] for k in range(4)]
    total = scores[0] + scores[1] + scores[2] + scores[3]
    slots = lax.broadcasted_iota(jnp.int32, (TOK, 512), 1)
    for j in range(ALL_SLOTS // 512):
        weighted = jnp.zeros((TOK, 512), F32)
        for k in range(4):
            here = (place[k] - j * 512 == slots).astype(F32)
            weighted = weighted + here * (ROUTE_SCALE * scores[k] / total)
        high = weighted.astype(BF16)
        high_ref[:, j * 512 : (j + 1) * 512] = high
        low_ref[:, j * 512 : (j + 1) * 512] = (weighted - high.astype(F32)).astype(BF16)


def dispatch_kernel(pick_ref, in_ref, residual_ref, out_ref, mid_ref):
    total = residual_ref[...].astype(F32)
    for s in range(4):
        total = total + in_ref[s].astype(F32)
    mid = total.astype(BF16)
    mid_ref[...] = mid
    for j in range(4):
        rows = pl.ds(j * SLOTS, SLOTS)
        picked = jnp.dot(pick_ref[rows, :], mid, preferred_element_type=F32)
        out_ref[rows, :] = picked.astype(BF16)


def expert_kernel(ready, ids_ref, x0, x1, x2, x3, gain_ref, gate_ref, up_ref, out_ref, wide_ref, rows_ref):
    part = ids_ref[0]
    squares = jnp.zeros((SLOTS, 128), F32)
    for m, x_ref in enumerate((x0, x1, x2, x3)):
        for s in range(32):
            wide_ref[m, s * PITCH : s * PITCH + 48, :] = x_ref[s * 48 : (s + 1) * 48, :].astype(F32)
    for m in range(4):
        for q in range(4):
            slab = q * 4 + (part ^ m)
            tile = jnp.concatenate(
                [wide_ref[m, pl.ds(q * MOST + r, 32, stride=PITCH), :] for r in range(MOST)], axis=0
            )
            squares = squares + tile * tile
            scaled = (tile * gain_ref[pl.ds(slab, 1), :]).astype(BF16)
            rows_ref[:, pl.ds(pl.multiple_of(slab * 128, 128), 128)] = scaled
    scale = lax.rsqrt(jnp.sum(squares, axis=1, keepdims=True) * (1.0 / D) + EPSILON)
    ready()
    gate = jnp.dot(rows_ref[...], gate_ref[...], preferred_element_type=F32) * scale
    up = jnp.dot(rows_ref[...], up_ref[...], preferred_element_type=F32) * scale
    out_ref[...] = (jax.nn.silu(gate) * up).astype(BF16)


def gain_kernel(in_ref, out_ref):
    out_ref[...] = in_ref[...].astype(F32)


def down_kernel(h0, h1, h2, h3, d0, d1, d2, d3, out_ref, wide_ref):
    total = jnp.zeros((SLOTS, 512), F32)
    for h_ref, d_ref in ((h0, d0), (h1, d1), (h2, d2), (h3, d3)):
        total = total + jnp.dot(h_ref[...], d_ref[0:256, :], preferred_element_type=F32)
    for q in range(4):
        for r in range(MOST):
            wide_ref[pl.ds(q * MOST + r, 32, stride=PITCH), :] = total[
                r * 32 : (r + 1) * 32, q * 128 : (q + 1) * 128
            ]
    for s in range(32):
        out_ref[s * 48 : (s + 1) * 48, :] = wide_ref[s * PITCH : s * PITCH + 48, :].astype(BF16)


def blocks_kernel(ids_ref, project_ref, *out_refs):
    part = ids_ref[0]
    for m, out_ref in enumerate(out_refs):
        for q in range(4):
            at = pl.multiple_of((q * 4 + (part ^ m)) * 256, 256)
            out_ref[:, q * 128 : (q + 1) * 128] = project_ref[pl.ds(at, 256), :]


def parts_kernel(ids_ref, down_ref, shared_ref, *out_refs):
    part = ids_ref[0]
    for m, out_ref in enumerate(out_refs):
        for q in range(4):
            lanes = slice(q * 128, (q + 1) * 128)
            columns = pl.ds(pl.multiple_of((q * 4 + (part ^ m)) * 128, 128), 128)
            out_ref[0:256, lanes] = down_ref[:, columns]
            out_ref[256:320, lanes] = shared_ref[:, columns]


def shared_in_kernel(ids_ref, m0, m1, m2, m3, w0, w1, w2, w3, gain_ref, out_ref, weight_ref, mid_ref):
    part, group = ids_ref[0], ids_ref[1]
    for m, w_ref in enumerate((w0, w1, w2, w3)):
        at = (part ^ m) * 32
        weight_ref[pl.ds(pl.multiple_of(at, 32), 32), :] = w_ref[256:288, :]
        weight_ref[pl.ds(pl.multiple_of(at + 128, 32), 32), :] = w_ref[288:320, :]
    for d, m_ref in enumerate((m0, m1, m2, m3)):
        mid_ref[(group - d) & 3] = m_ref[...]
    squares = jnp.zeros((TOK, 128), F32)
    pre = jnp.zeros((TOK, 256), F32)
    for q in range(4):
        tile = mid_ref[q].astype(F32)
        squares = squares + tile * tile
        scaled = (tile * gain_ref[pl.ds(q * 4 + part, 1), :]).astype(BF16)
        pre = pre + nt(scaled, weight_ref[:, q * 128 : (q + 1) * 128])
    ssq = jnp.sum(squares, axis=1, keepdims=True)
    high = ssq.astype(BF16).astype(F32)
    lane = lax.broadcasted_iota(jnp.int32, (TOK, 128), 1)
    tail = jnp.where(lane == 0, high, jnp.where(lane == 1, ssq - high, 0.0)).astype(BF16)
    out_ref[:, 0:256] = pre.astype(BF16)
    out_ref[:, 256:384] = tail


def shared_hidden_kernel(r0, r1, r2, r3, out_ref):
    total = sum(r[...].astype(F32) for r in (r0, r1, r2, r3))
    ssq = jnp.sum(total[:, 256:384], axis=1, keepdims=True)
    scale = lax.rsqrt(ssq * (1.0 / D) + EPSILON)
    hidden = jax.nn.silu(total[:, 0:128] * scale) * (total[:, 128:256] * scale)
    out_ref[...] = hidden.astype(BF16)


def ahead_kernel(ids_ref, h0, h1, h2, h3, down_ref, mid_ref, out_ref):
    group = ids_ref[1]
    total = mid_ref[...].astype(F32)
    for d, h in enumerate((h0, h1, h2, h3)):
        at = pl.multiple_of(((group - d) & 3) * 128, 128)
        total = total + jnp.dot(
            h[...], down_ref[pl.ds(at, 128), :], preferred_element_type=F32
        )
    out_ref[...] = total


def final_kernel(back_ref, high_ref, low_ref, ahead_ref, out_ref):
    back = back_ref[...]
    total = ahead_ref[...] + jnp.dot(high_ref[...], back, preferred_element_type=F32)
    total = total + jnp.dot(low_ref[...], back, preferred_element_type=F32)
    out_ref[...] = total.astype(BF16)


def exchange(value, axes):
    return lax.all_to_all(value, axes, split_axis=0, concat_axis=0, tiled=True)


def moved(value, axes, target):
    count = lax.axis_size(axes)
    return lax.ppermute(value, axes, [(i, target(i) % count) for i in range(count)])


def shifted(values, axes):
    return [moved(v, axes, lambda i, d=d: i + d) for d, v in enumerate(values, 1)]


def swapped(value, axis):
    return moved(value, axis, lambda i: i ^ 1)


def grouped(values):
    return [moved(v, GROUP, lambda i, m=m: i ^ m) for m, v in enumerate(values, 1)]


def body(
    queries,
    key_matrix,
    value_matrix,
    output_gate_preactivation,
    decay_preactivation,
    extra_log_decay,
    head_norm_gain,
    output_projection,
    residual,
    feedforward_gain,
    routing,
    router_score,
    expert_gate_weight,
    expert_up_weight,
    expert_down_weight,
    shared_expert_gate,
    shared_expert_up,
    shared_expert_down,
):
    ids = jnp.stack([lax.axis_index(a) for a in (GROUP, "yg")]).astype(jnp.int32)
    gain = call(gain_kernel, ((16, 128), F32), feedforward_gain.reshape(16, 128))
    head_gain = head_norm_gain.reshape(1, DV)
    extra = extra_log_decay.reshape(2, 128)
    whole = (0, TOK)

    payload = call(
        state_kernel, ((32, 16, DK), BF16),
        key_matrix, value_matrix, decay_preactivation, extra, fetch=(whole, whole, whole, (0, 2)), limit=60,
    )
    states = exchange(payload, SP)
    local, start = call(
        local_kernel, [((TOK, DV), F32), ((TOK, DK), F32)],
        queries, key_matrix, value_matrix, decay_preactivation, extra,
        fetch=(whole, whole, whole, whole, (0, 2)), limit=60,
    )
    pick = call(pick_kernel, ((ALL_SLOTS, TOK), BF16), routing)
    high, low = call(
        weigh_kernel, [((TOK, ALL_SLOTS), BF16), ((TOK, ALL_SLOTS), BF16)], routing, router_score
    )
    shared_in = jnp.concatenate([shared_expert_gate.T, shared_expert_up.T], axis=0)
    own_block, *far_blocks = call(
        blocks_kernel, [((256, 512), BF16)] * 4, ids, output_projection, smem=1,
    )
    blocks = [own_block] + grouped(far_blocks)
    own_part, *far_parts = call(
        parts_kernel, [((320, 512), BF16)] * 4, ids, expert_down_weight, shared_in, smem=1,
    )
    parts = [own_part] + grouped(far_parts)

    entering = exchange(call(scan_kernel, ((32, 8, DK), BF16), states), SP)
    head_rows = call(
        head_kernel, ((4, TOK, DV), BF16),
        entering.reshape(DV, DK), head_gain, local, start, output_gate_preactivation,
        fetch=(whole,) * 3,
    )
    partial = call(
        project_kernel, ((4, TOK, 128), BF16),
        ids, exchange(head_rows, "yg"), *blocks, smem=1, fetch=(whole,) * 4,
    )
    outgoing, mid = call(
        dispatch_kernel, [((ALL_SLOTS, 128), BF16), ((TOK, 128), BF16)],
        pick, exchange(partial, GROUP), residual,
    )
    own = exchange(outgoing.reshape(128, 3, 4, 128), SPG).reshape(ALL_SLOTS, 128)
    mids = [mid] + shifted([mid] * 3, "yg")

    across = swapped(own, "yn")
    beside = swapped(own, "c")
    far = swapped(across, "c")
    pre = call(
        shared_in_kernel, ((TOK, 384), BF16), ids, *mids, *parts, gain, smem=1,
        scratch=[pltpu.VMEM((256, 512), BF16), pltpu.VMEM((4, TOK, 128), BF16)],
    )
    pre = [pre] + grouped([pre] * 3)
    routed = call(
        expert_kernel, ((SLOTS, 256), BF16),
        ids, own, beside, across, far, gain, expert_gate_weight, expert_up_weight,
        smem=1, fetch=((0, D), (0, D)), late=True,
        scratch=[pltpu.VMEM((4, 32 * PITCH, 128), F32), pltpu.VMEM((SLOTS, D), BF16)],
    )
    routed_across = swapped(routed, "yn")
    routed_beside = swapped(routed, "c")
    routed_far = swapped(routed_across, "c")
    expert_out = call(
        down_kernel, ((ALL_SLOTS, 128), BF16),
        routed, routed_beside, routed_across, routed_far, *parts,
        scratch=[pltpu.VMEM((32 * PITCH, 128), F32)],
    )
    back = exchange(expert_out.reshape(128, 3, 4, 128), SPG).reshape(ALL_SLOTS, 128)
    hidden = call(shared_hidden_kernel, ((TOK, 128), BF16), *pre)
    hidden = [hidden] + shifted([hidden] * 3, "yg")
    ahead = call(
        ahead_kernel, ((TOK, 128), F32), ids, *hidden, shared_expert_down, mid, smem=1,
    )
    return call(final_kernel, ((TOK, 128), BF16), back, high, low, ahead)


def solution(mesh):
    finer = Mesh(mesh.devices.reshape(8, 4, 4, 2, 2), ("z", "x", "yg", "yn", "c"))
    in_specs = (
        P(SP, TP),
        P(SP, TP),
        P(SP, TP),
        P(SP, TP),
        P(SP, TP),
        P(SP, TP),
        P(),
        P(None, TP),
        P(SP, TP),
        P(),
        P(SP, None),
        P(SP, None),
        P(None, SP + TP),
        P(None, SP + TP),
        P(SP + TP, None),
        P(None, TP),
        P(None, TP),
        P(None, TP),
    )
    return jax.shard_map(body, mesh=finer, in_specs=in_specs, out_specs=P(SP, TP), check_vma=False)
```

```python
import jax
import jax.numpy as jnp
from jax import lax
from jax.experimental import pallas as pl
from jax.experimental.pallas import tpu as pltpu
from jax.sharding import Mesh
from jax.sharding import PartitionSpec as P

DK = 128
DV = 256
BLOCK = 64
TOK = 256
MOST = 12
SLOTS = 384
ALL_SLOTS = 1536
PITCH = 56
D = 2048
SP = ("z", "x")
SPG = ("z", "x", "yg")
TP = ("yg", "yn", "c")
GROUP = ("yn", "c")
F32 = jnp.float32
BF16 = jnp.bfloat16
HIGHEST = lax.Precision.HIGHEST
EPSILON = 1e-06
ROUTE_SCALE = 2.5
GATE_TEMPER = 16.0
VMEM = pl.BlockSpec(memory_space=pltpu.VMEM)
SMEM = pl.BlockSpec(memory_space=pltpu.SMEM)


def call(kernel, outs, *args, scratch=(), smem=0, fetch=(), late=False, limit=24):
    single = not isinstance(outs, list)
    shapes = [jax.ShapeDtypeStruct(s, t) for s, t in ([outs] if single else outs)]
    n_in, n_out, n_scratch, n_fetch = len(args), len(shapes), len(scratch), len(fetch)
    kept = n_in - n_fetch
    buffers = []
    for arg, rows in zip(args[kept:], fetch, strict=True):
        buffers.append(pltpu.VMEM((rows[1], *arg.shape[1:]), arg.dtype))

    def fetching(*refs):
        sources, results = refs[kept:n_in], refs[n_in : n_in + n_out]
        own = refs[n_in + n_out : n_in + n_out + n_scratch]
        held, sems = refs[n_in + n_out + n_scratch : -1], refs[-1]
        copies = [
            pltpu.make_async_copy(src.at[pl.ds(rows[0], rows[1])], dst, sems.at[i])
            for i, (src, dst, rows) in enumerate(zip(sources, held, fetch, strict=True))
        ]
        for copy in copies:
            copy.start()

        def ready():
            for copy in copies:
                copy.wait()

        if late:
            kernel(ready, *refs[:kept], *held, *results, *own)
        else:
            ready()
            kernel(*refs[:kept], *held, *results, *own)

    extra = buffers + [pltpu.SemaphoreType.DMA((n_fetch,))] if fetch else []
    any_spec = pl.BlockSpec(memory_space=pl.ANY)
    got = pl.pallas_call(
        fetching if fetch else kernel,
        out_shape=shapes,
        in_specs=[SMEM] * smem + [VMEM] * (kept - smem) + [any_spec] * n_fetch,
        out_specs=[VMEM] * n_out,
        scratch_shapes=list(scratch) + extra,
        compiler_params=pltpu.CompilerParams(vmem_limit_bytes=limit * 2**20),
        cost_estimate=pl.CostEstimate(
            flops=1000000, bytes_accessed=1000000, transcendentals=0
        ),
    )(*args)
    return got[0] if single else got


def nt(a, b, **kw):
    return lax.dot_general(
        a, b, (((1,), (1,)), ((), ())), preferred_element_type=F32, **kw
    )


def split(value, count):
    pieces = []
    for _ in range(count):
        piece = value.astype(BF16)
        pieces.append(piece)
        value = value - piece.astype(F32)
    return pieces


def dot(a, b):
    return jnp.dot(a, b, preferred_element_type=F32)


def decays(decay_ref, extra_ref):
    raw = decay_ref[...].astype(F32)
    logs = jax.nn.log_sigmoid(raw) / GATE_TEMPER
    rows = lax.broadcasted_iota(jnp.int32, (BLOCK, BLOCK), 0)
    cols = lax.broadcasted_iota(jnp.int32, (BLOCK, BLOCK), 1)
    lower = (rows >= cols).astype(F32).astype(BF16)
    wide_rows = lax.broadcasted_iota(jnp.int32, (BLOCK, 128), 0)
    wide_cols = lax.broadcasted_iota(jnp.int32, (BLOCK, 128), 1)
    ones = jnp.ones((128, DK), BF16)
    inside = []
    for b in range(TOK // BLOCK):
        at = wide_cols - (b % 2) * BLOCK
        extra = jnp.where((at >= 0) & (at <= wide_rows), extra_ref[b // 2 : b // 2 + 1, :], 0.0)
        total = sum(dot(lower, piece) for piece in split(logs[b * BLOCK : (b + 1) * BLOCK], 3))
        inside.append(total + sum(dot(piece, ones) for piece in split(extra, 3)))
    return inside


def block_states(inside, key_ref, value_ref):
    state = jnp.zeros((DV, DK), F32)
    states = []
    total = jnp.zeros((1, DK), F32)
    for b, cum in enumerate(inside):
        states.append(state)
        rows = pl.ds(b * BLOCK, BLOCK)
        end = cum[BLOCK - 1 : BLOCK]
        key_end = key_ref[rows, :].astype(F32) * jnp.exp(end - cum)
        value = value_ref[rows, :].astype(F32)
        fresh = jnp.dot(value.T, key_end, precision=HIGHEST, preferred_element_type=F32)
        state = jnp.exp(end) * state + fresh
        total = total + end
    return states, state, total


def state_kernel(key_ref, value_ref, decay_ref, extra_ref, out_ref):
    inside = decays(decay_ref, extra_ref)
    later = jnp.zeros((1, DK), F32)
    scaled = []
    for cum in reversed(inside):
        end = cum[BLOCK - 1 : BLOCK]
        scaled.insert(0, jnp.exp(end - cum + later))
        later = later + end
    key_end = key_ref[...].astype(F32) * jnp.concatenate(scaled, axis=0)
    value_t = value_ref[...].astype(F32).T.astype(BF16)
    state = sum(dot(value_t, piece) for piece in split(key_end, 3))
    out_ref[:, 0:8, :] = state.reshape(32, 8, DK).astype(BF16)
    decay = jnp.exp(later)
    high = decay.astype(BF16).astype(F32)
    row = lax.broadcasted_iota(jnp.int32, (8, DK), 0)
    tail = jnp.where(row == 0, high, jnp.where(row == 1, decay - high, 0.0))
    out_ref[:, 8:16, :] = jnp.broadcast_to(tail[None], (32, 8, DK)).astype(BF16)


def scan_kernel(in_ref, out_ref):
    state = jnp.zeros((8, DK), F32)
    for s in range(32):
        out_ref[s] = state.astype(BF16)
        block = in_ref[s].astype(F32)
        decay = block[8:9] + block[9:10]
        state = decay * state + block[0:8]


def local_kernel(query_ref, key_ref, value_ref, decay_ref, extra_ref, local_ref, start_ref):
    inside = decays(decay_ref, extra_ref)
    states, _, _ = block_states(inside, key_ref, value_ref)
    rows_at = lax.broadcasted_iota(jnp.int32, (BLOCK, BLOCK), 0)
    cols_at = lax.broadcasted_iota(jnp.int32, (BLOCK, BLOCK), 1)
    before = jnp.zeros((1, DK), F32)
    for b, cum in enumerate(inside):
        rows = pl.ds(b * BLOCK, BLOCK)
        query = query_ref[rows, :].astype(F32) * DK ** (-0.5)
        key = key_ref[rows, :].astype(F32)
        value = value_ref[rows, :].astype(F32)
        query_decay = query * jnp.exp(cum)
        scores = nt(query_decay, key * jnp.exp(-cum), precision=HIGHEST)
        scores = jnp.where(rows_at >= cols_at, scores, 0.0)
        mixed = jnp.dot(scores, value, precision=HIGHEST, preferred_element_type=F32)
        if b > 0:
            mixed = mixed + nt(query_decay, states[b], precision=HIGHEST)
        local_ref[rows, :] = mixed
        start_ref[rows, :] = query * jnp.exp(cum + before)
        before = before + cum[BLOCK - 1 : BLOCK]


def head_kernel(gain_ref, enter_ref, local_ref, start_ref, gate_ref, out_ref):
    enter = enter_ref[...]
    mixed = local_ref[...] + sum(nt(piece, enter) for piece in split(start_ref[...], 3))
    scale = lax.rsqrt(jnp.mean(mixed * mixed, axis=-1, keepdims=True) + EPSILON)
    gate = jax.nn.silu(gate_ref[...].astype(F32))
    rows = (mixed * scale * gain_ref[...].astype(F32) * gate).astype(BF16)
    for dest in range(4):
        out_ref[dest] = rows


def project_kernel(ids_ref, heads_ref, w0, w1, w2, w3, out_ref):
    part = ids_ref[0]
    for m in (0, 2):
        pair = ((w0, w1), None, (w2, w3))[m]
        total = jnp.zeros((TOK, 256), F32)
        for h in range(4):
            lanes = slice(h * 128, (h + 1) * 128)
            weight = jnp.concatenate([w[:, lanes] for w in pair], axis=1)
            total = total + jnp.dot(heads_ref[h], weight, preferred_element_type=F32)
        out_ref[part ^ m] = total[:, :128].astype(BF16)
        out_ref[part ^ (m + 1)] = total[:, 128:].astype(BF16)


def places(routing_ref):
    experts = lax.broadcasted_iota(jnp.int32, (TOK, 128), 1)
    hot = [(routing_ref[:, k : k + 1] == experts).astype(F32) for k in range(4)]
    named = hot[0] + hot[1] + hot[2] + hot[3]
    rows = lax.broadcasted_iota(jnp.int32, (TOK, TOK), 0)
    cols = lax.broadcasted_iota(jnp.int32, (TOK, TOK), 1)
    earlier = (rows > cols).astype(BF16)
    ranks = jnp.dot(earlier, named.astype(BF16), preferred_element_type=F32)
    return [
        routing_ref[:, k : k + 1] * MOST
        + jnp.sum(hot[k] * ranks, axis=1, keepdims=True).astype(jnp.int32)
        for k in range(4)
    ]


def pick_kernel(routing_ref, pick_ref):
    place = places(routing_ref)
    slots = lax.broadcasted_iota(jnp.int32, (TOK, 512), 1)
    for j in range(ALL_SLOTS // 512):
        picked = jnp.zeros((TOK, 512), F32)
        for k in range(4):
            picked = picked + (place[k] - j * 512 == slots).astype(F32)
        pick_ref[j * 512 : (j + 1) * 512, :] = picked.T.astype(BF16)


def weigh_kernel(routing_ref, score_ref, high_ref, low_ref):
    place = places(routing_ref)
    scores = [score_ref[:, k : k + 1] for k in range(4)]
    total = scores[0] + scores[1] + scores[2] + scores[3]
    slots = lax.broadcasted_iota(jnp.int32, (TOK, 512), 1)
    for j in range(ALL_SLOTS // 512):
        weighted = jnp.zeros((TOK, 512), F32)
        for k in range(4):
            here = (place[k] - j * 512 == slots).astype(F32)
            weighted = weighted + here * (ROUTE_SCALE * scores[k] / total)
        high = weighted.astype(BF16)
        high_ref[:, j * 512 : (j + 1) * 512] = high
        low_ref[:, j * 512 : (j + 1) * 512] = (weighted - high.astype(F32)).astype(BF16)


def dispatch_kernel(pick_ref, in_ref, residual_ref, out_ref, mid_ref):
    total = residual_ref[...].astype(F32)
    for s in range(4):
        total = total + in_ref[s].astype(F32)
    mid = total.astype(BF16)
    mid_ref[...] = mid
    for j in range(4):
        rows = pl.ds(j * SLOTS, SLOTS)
        picked = jnp.dot(pick_ref[rows, :], mid, preferred_element_type=F32)
        out_ref[rows, :] = picked.astype(BF16)


def expert_kernel(ready, ids_ref, x0, x1, x2, x3, gain_ref, gate_ref, up_ref, out_ref, wide_ref, rows_ref):
    part = ids_ref[0]
    squares = jnp.zeros((SLOTS, 128), F32)
    for m, x_ref in enumerate((x0, x1, x2, x3)):
        for s in range(32):
            wide_ref[m, s * PITCH : s * PITCH + 48, :] = x_ref[s * 48 : (s + 1) * 48, :].astype(F32)
    for m in range(4):
        for q in range(4):
            slab = q * 4 + (part ^ m)
            tile = jnp.concatenate(
                [wide_ref[m, pl.ds(q * MOST + r, 32, stride=PITCH), :] for r in range(MOST)], axis=0
            )
            squares = squares + tile * tile
            scaled = (tile * gain_ref[pl.ds(slab, 1), :]).astype(BF16)
            rows_ref[:, pl.ds(pl.multiple_of(slab * 128, 128), 128)] = scaled
    scale = lax.rsqrt(jnp.sum(squares, axis=1, keepdims=True) * (1.0 / D) + EPSILON)
    ready()
    gate = jnp.dot(rows_ref[...], gate_ref[...], preferred_element_type=F32) * scale
    up = jnp.dot(rows_ref[...], up_ref[...], preferred_element_type=F32) * scale
    out_ref[...] = (jax.nn.silu(gate) * up).astype(BF16)


def gain_kernel(in_ref, out_ref):
    out_ref[...] = in_ref[...].astype(F32)


def down_kernel(h0, h1, h2, h3, d0, d1, d2, d3, out_ref, wide_ref):
    total = jnp.zeros((SLOTS, 512), F32)
    for h_ref, d_ref in ((h0, d0), (h1, d1), (h2, d2), (h3, d3)):
        total = total + jnp.dot(h_ref[...], d_ref[256:512, :], preferred_element_type=F32)
    for q in range(4):
        for r in range(MOST):
            wide_ref[pl.ds(q * MOST + r, 32, stride=PITCH), :] = total[
                r * 32 : (r + 1) * 32, q * 128 : (q + 1) * 128
            ]
    for s in range(32):
        out_ref[s * 48 : (s + 1) * 48, :] = wide_ref[s * PITCH : s * PITCH + 48, :].astype(BF16)


def parts_kernel(ids_ref, project_ref, down_ref, shared_ref, *out_refs):
    part = ids_ref[0]
    for m, out_ref in enumerate(out_refs):
        for q in range(4):
            slab = q * 4 + (part ^ m)
            lanes = slice(q * 128, (q + 1) * 128)
            out_ref[0:256, lanes] = project_ref[pl.ds(pl.multiple_of(slab * 256, 256), 256), :]
            columns = pl.ds(pl.multiple_of(slab * 128, 128), 128)
            out_ref[256:512, lanes] = down_ref[:, columns]
            out_ref[512:576, lanes] = shared_ref[:, columns]


def shared_in_kernel(ids_ref, m0, m1, m2, m3, w0, w1, w2, w3, gain_ref, out_ref, weight_ref, mid_ref):
    part, group = ids_ref[0], ids_ref[1]
    for m, w_ref in enumerate((w0, w1, w2, w3)):
        at = (part ^ m) * 32
        weight_ref[pl.ds(pl.multiple_of(at, 32), 32), :] = w_ref[512:544, :]
        weight_ref[pl.ds(pl.multiple_of(at + 128, 32), 32), :] = w_ref[544:576, :]
    for d, m_ref in enumerate((m0, m1, m2, m3)):
        mid_ref[(group - d) & 3] = m_ref[...]
    squares = jnp.zeros((TOK, 128), F32)
    pre = jnp.zeros((TOK, 256), F32)
    for q in range(4):
        tile = mid_ref[q].astype(F32)
        squares = squares + tile * tile
        scaled = (tile * gain_ref[pl.ds(q * 4 + part, 1), :]).astype(BF16)
        pre = pre + nt(scaled, weight_ref[:, q * 128 : (q + 1) * 128])
    ssq = jnp.sum(squares, axis=1, keepdims=True)
    high = ssq.astype(BF16).astype(F32)
    lane = lax.broadcasted_iota(jnp.int32, (TOK, 128), 1)
    tail = jnp.where(lane == 0, high, jnp.where(lane == 1, ssq - high, 0.0)).astype(BF16)
    out_ref[:, 0:256] = pre.astype(BF16)
    out_ref[:, 256:384] = tail


def shared_hidden_kernel(r0, r1, r2, r3, out_ref):
    total = sum(r[...].astype(F32) for r in (r0, r1, r2, r3))
    ssq = jnp.sum(total[:, 256:384], axis=1, keepdims=True)
    scale = lax.rsqrt(ssq * (1.0 / D) + EPSILON)
    hidden = jax.nn.silu(total[:, 0:128] * scale) * (total[:, 128:256] * scale)
    out_ref[...] = hidden.astype(BF16)


def ahead_kernel(ids_ref, h0, h1, h2, h3, down_ref, mid_ref, out_ref):
    group = ids_ref[1]
    total = mid_ref[...].astype(F32)
    for d, h in enumerate((h0, h1, h2, h3)):
        at = pl.multiple_of(((group - d) & 3) * 128, 128)
        total = total + jnp.dot(
            h[...], down_ref[pl.ds(at, 128), :], preferred_element_type=F32
        )
    out_ref[...] = total


def final_kernel(back_ref, high_ref, low_ref, ahead_ref, out_ref):
    back = back_ref[...]
    total = ahead_ref[...] + jnp.dot(high_ref[...], back, preferred_element_type=F32)
    total = total + jnp.dot(low_ref[...], back, preferred_element_type=F32)
    out_ref[...] = total.astype(BF16)


def exchange(value, axes):
    return lax.all_to_all(value, axes, split_axis=0, concat_axis=0, tiled=True)


def moved(value, axes, target):
    count = lax.axis_size(axes)
    return lax.ppermute(value, axes, [(i, target(i) % count) for i in range(count)])


def shifted(values, axes):
    return [moved(v, axes, lambda i, d=d: i + d) for d, v in enumerate(values, 1)]


def swapped(value, axis):
    return moved(value, axis, lambda i: i ^ 1)


def grouped(values):
    return [moved(v, GROUP, lambda i, m=m: i ^ m) for m, v in enumerate(values, 1)]


def body(
    queries,
    key_matrix,
    value_matrix,
    output_gate_preactivation,
    decay_preactivation,
    extra_log_decay,
    head_norm_gain,
    output_projection,
    residual,
    feedforward_gain,
    routing,
    router_score,
    expert_gate_weight,
    expert_up_weight,
    expert_down_weight,
    shared_expert_gate,
    shared_expert_up,
    shared_expert_down,
):
    ids = jnp.stack([lax.axis_index(a) for a in (GROUP, "yg")]).astype(jnp.int32)
    gain = call(gain_kernel, ((16, 128), F32), feedforward_gain.reshape(16, 128))
    head_gain = head_norm_gain.reshape(1, DV)
    extra = extra_log_decay.reshape(2, 128)
    whole = (0, TOK)

    payload = call(
        state_kernel, ((32, 16, DK), BF16),
        key_matrix, value_matrix, decay_preactivation, extra, fetch=(whole, whole, whole, (0, 2)), limit=60,
    )
    states = exchange(payload, SP)
    local, start = call(
        local_kernel, [((TOK, DV), F32), ((TOK, DK), F32)],
        queries, key_matrix, value_matrix, decay_preactivation, extra,
        fetch=(whole, whole, whole, whole, (0, 2)), limit=60,
    )
    pick = call(pick_kernel, ((ALL_SLOTS, TOK), BF16), routing)
    high, low = call(
        weigh_kernel, [((TOK, ALL_SLOTS), BF16), ((TOK, ALL_SLOTS), BF16)], routing, router_score
    )
    shared_in = jnp.concatenate([shared_expert_gate.T, shared_expert_up.T], axis=0)
    own_part, *far_parts = call(
        parts_kernel, [((576, 512), BF16)] * 4,
        ids, output_projection, expert_down_weight, shared_in, smem=1,
    )
    parts = [own_part] + grouped(far_parts)

    entering = exchange(call(scan_kernel, ((32, 8, DK), BF16), states), SP)
    head_rows = call(
        head_kernel, ((4, TOK, DV), BF16),
        head_gain, entering.reshape(DV, DK), local, start, output_gate_preactivation,
        fetch=(whole,) * 4, limit=60,
    )
    partial = call(
        project_kernel, ((4, TOK, 128), BF16),
        ids, exchange(head_rows, "yg"), *parts, smem=1, fetch=(whole,) * 4,
    )
    outgoing, mid = call(
        dispatch_kernel, [((ALL_SLOTS, 128), BF16), ((TOK, 128), BF16)],
        pick, exchange(partial, GROUP), residual,
    )
    own = exchange(outgoing.reshape(128, 3, 4, 128), SPG).reshape(ALL_SLOTS, 128)
    mids = [mid] + shifted([mid] * 3, "yg")

    across = swapped(own, "yn")
    beside = swapped(own, "c")
    far = swapped(across, "c")
    pre = call(
        shared_in_kernel, ((TOK, 384), BF16), ids, *mids, *parts, gain, smem=1,
        scratch=[pltpu.VMEM((256, 512), BF16), pltpu.VMEM((4, TOK, 128), BF16)],
    )
    pre = [pre] + grouped([pre] * 3)
    routed = call(
        expert_kernel, ((SLOTS, 256), BF16),
        ids, own, beside, across, far, gain, expert_gate_weight, expert_up_weight,
        smem=1, fetch=((0, D), (0, D)), late=True,
        scratch=[pltpu.VMEM((4, 32 * PITCH, 128), F32), pltpu.VMEM((SLOTS, D), BF16)],
    )
    routed_across = swapped(routed, "yn")
    routed_beside = swapped(routed, "c")
    routed_far = swapped(routed_across, "c")
    expert_out = call(
        down_kernel, ((ALL_SLOTS, 128), BF16),
        routed, routed_beside, routed_across, routed_far, *parts,
        scratch=[pltpu.VMEM((32 * PITCH, 128), F32)],
    )
    back = exchange(expert_out.reshape(128, 3, 4, 128), SPG).reshape(ALL_SLOTS, 128)
    hidden = call(shared_hidden_kernel, ((TOK, 128), BF16), *pre)
    hidden = [hidden] + shifted([hidden] * 3, "yg")
    ahead = call(
        ahead_kernel, ((TOK, 128), F32), ids, *hidden, shared_expert_down, mid, smem=1,
    )
    return call(final_kernel, ((TOK, 128), BF16), back, high, low, ahead)


def solution(mesh):
    finer = Mesh(mesh.devices.reshape(8, 4, 4, 2, 2), ("z", "x", "yg", "yn", "c"))
    in_specs = (
        P(SP, TP),
        P(SP, TP),
        P(SP, TP),
        P(SP, TP),
        P(SP, TP),
        P(SP, TP),
        P(),
        P(None, TP),
        P(SP, TP),
        P(),
        P(SP, None),
        P(SP, None),
        P(None, SP + TP),
        P(None, SP + TP),
        P(SP + TP, None),
        P(None, TP),
        P(None, TP),
        P(None, TP),
    )
    return jax.shard_map(body, mesh=finer, in_specs=in_specs, out_specs=P(SP, TP), check_vma=False)
```

```python
import jax
import jax.numpy as jnp
from jax import lax
from jax.experimental import pallas as pl
from jax.experimental.pallas import tpu as pltpu
from jax.sharding import Mesh
from jax.sharding import PartitionSpec as P

DK = 128
DV = 256
BLOCK = 64
TOK = 256
MOST = 12
SLOTS = 384
ALL_SLOTS = 1536
PITCH = 56
D = 2048
SP = ("z", "x")
SPG = ("z", "x", "yg")
TP = ("yg", "yn", "c")
GROUP = ("yn", "c")
F32 = jnp.float32
BF16 = jnp.bfloat16
HIGHEST = lax.Precision.HIGHEST
EPSILON = 1e-06
ROUTE_SCALE = 2.5
GATE_TEMPER = 16.0
VMEM = pl.BlockSpec(memory_space=pltpu.VMEM)
SMEM = pl.BlockSpec(memory_space=pltpu.SMEM)


def call(kernel, outs, *args, scratch=(), smem=0, fetch=(), late=False, limit=24):
    single = not isinstance(outs, list)
    shapes = [jax.ShapeDtypeStruct(s, t) for s, t in ([outs] if single else outs)]
    n_in, n_out, n_scratch, n_fetch = len(args), len(shapes), len(scratch), len(fetch)
    kept = n_in - n_fetch
    buffers = []
    for arg, rows in zip(args[kept:], fetch, strict=True):
        buffers.append(pltpu.VMEM((rows[1], *arg.shape[1:]), arg.dtype))

    def fetching(*refs):
        sources, results = refs[kept:n_in], refs[n_in : n_in + n_out]
        own = refs[n_in + n_out : n_in + n_out + n_scratch]
        held, sems = refs[n_in + n_out + n_scratch : -1], refs[-1]
        copies = [
            pltpu.make_async_copy(src.at[pl.ds(rows[0], rows[1])], dst, sems.at[i])
            for i, (src, dst, rows) in enumerate(zip(sources, held, fetch, strict=True))
        ]
        for copy in copies:
            copy.start()

        def ready():
            for copy in copies:
                copy.wait()

        if late:
            kernel(ready, *refs[:kept], *held, *results, *own)
        else:
            ready()
            kernel(*refs[:kept], *held, *results, *own)

    extra = buffers + [pltpu.SemaphoreType.DMA((n_fetch,))] if fetch else []
    any_spec = pl.BlockSpec(memory_space=pl.ANY)
    got = pl.pallas_call(
        fetching if fetch else kernel,
        out_shape=shapes,
        in_specs=[SMEM] * smem + [VMEM] * (kept - smem) + [any_spec] * n_fetch,
        out_specs=[VMEM] * n_out,
        scratch_shapes=list(scratch) + extra,
        compiler_params=pltpu.CompilerParams(vmem_limit_bytes=limit * 2**20),
        cost_estimate=pl.CostEstimate(
            flops=1000000, bytes_accessed=1000000, transcendentals=0
        ),
    )(*args)
    return got[0] if single else got


def nt(a, b, **kw):
    return lax.dot_general(
        a, b, (((1,), (1,)), ((), ())), preferred_element_type=F32, **kw
    )


def split(value, count):
    pieces = []
    for _ in range(count):
        piece = value.astype(BF16)
        pieces.append(piece)
        value = value - piece.astype(F32)
    return pieces


def dot(a, b):
    return jnp.dot(a, b, preferred_element_type=F32)


def decays(decay_ref, extra_ref):
    raw = decay_ref[...].astype(F32)
    logs = jax.nn.log_sigmoid(raw) / GATE_TEMPER
    rows = lax.broadcasted_iota(jnp.int32, (BLOCK, BLOCK), 0)
    cols = lax.broadcasted_iota(jnp.int32, (BLOCK, BLOCK), 1)
    lower = (rows >= cols).astype(F32).astype(BF16)
    wide_rows = lax.broadcasted_iota(jnp.int32, (BLOCK, 128), 0)
    wide_cols = lax.broadcasted_iota(jnp.int32, (BLOCK, 128), 1)
    ones = jnp.ones((128, DK), BF16)
    inside = []
    for b in range(TOK // BLOCK):
        at = wide_cols - (b % 2) * BLOCK
        extra = jnp.where((at >= 0) & (at <= wide_rows), extra_ref[b // 2 : b // 2 + 1, :], 0.0)
        total = sum(dot(lower, piece) for piece in split(logs[b * BLOCK : (b + 1) * BLOCK], 3))
        inside.append(total + sum(dot(piece, ones) for piece in split(extra, 3)))
    return inside


def block_states(inside, key_ref, value_ref):
    state = jnp.zeros((DV, DK), F32)
    states = []
    total = jnp.zeros((1, DK), F32)
    for b, cum in enumerate(inside):
        states.append(state)
        rows = pl.ds(b * BLOCK, BLOCK)
        end = cum[BLOCK - 1 : BLOCK]
        key_end = key_ref[rows, :].astype(F32) * jnp.exp(end - cum)
        value = value_ref[rows, :].astype(F32)
        fresh = jnp.dot(value.T, key_end, precision=HIGHEST, preferred_element_type=F32)
        state = jnp.exp(end) * state + fresh
        total = total + end
    return states, state, total


def state_kernel(key_ref, value_ref, decay_ref, extra_ref, out_ref):
    inside = decays(decay_ref, extra_ref)
    later = jnp.zeros((1, DK), F32)
    scaled = []
    for cum in reversed(inside):
        end = cum[BLOCK - 1 : BLOCK]
        scaled.insert(0, jnp.exp(end - cum + later))
        later = later + end
    key_end = key_ref[...].astype(F32) * jnp.concatenate(scaled, axis=0)
    value_t = value_ref[...].astype(F32).T.astype(BF16)
    state = sum(dot(value_t, piece) for piece in split(key_end, 3))
    out_ref[:, 0:8, :] = state.reshape(32, 8, DK).astype(BF16)
    decay = jnp.exp(later)
    high = decay.astype(BF16).astype(F32)
    row = lax.broadcasted_iota(jnp.int32, (8, DK), 0)
    tail = jnp.where(row == 0, high, jnp.where(row == 1, decay - high, 0.0))
    out_ref[:, 8:16, :] = jnp.broadcast_to(tail[None], (32, 8, DK)).astype(BF16)


def scan_kernel(in_ref, out_ref):
    state = jnp.zeros((8, DK), F32)
    for s in range(32):
        out_ref[s] = state.astype(BF16)
        block = in_ref[s].astype(F32)
        decay = block[8:9] + block[9:10]
        state = decay * state + block[0:8]


def local_kernel(query_ref, key_ref, value_ref, decay_ref, extra_ref, local_ref, start_ref):
    inside = decays(decay_ref, extra_ref)
    states, _, _ = block_states(inside, key_ref, value_ref)
    rows_at = lax.broadcasted_iota(jnp.int32, (BLOCK, BLOCK), 0)
    cols_at = lax.broadcasted_iota(jnp.int32, (BLOCK, BLOCK), 1)
    before = jnp.zeros((1, DK), F32)
    for b, cum in enumerate(inside):
        rows = pl.ds(b * BLOCK, BLOCK)
        query = query_ref[rows, :].astype(F32) * DK ** (-0.5)
        key = key_ref[rows, :].astype(F32)
        value = value_ref[rows, :].astype(F32)
        query_decay = query * jnp.exp(cum)
        scores = nt(query_decay, key * jnp.exp(-cum), precision=HIGHEST)
        scores = jnp.where(rows_at >= cols_at, scores, 0.0)
        mixed = jnp.dot(scores, value, precision=HIGHEST, preferred_element_type=F32)
        if b > 0:
            mixed = mixed + nt(query_decay, states[b], precision=HIGHEST)
        local_ref[rows, :] = mixed
        start_ref[rows, :] = query * jnp.exp(cum + before)
        before = before + cum[BLOCK - 1 : BLOCK]


def head_kernel(enter_ref, gain_ref, local_ref, start_ref, gate_ref, out_ref):
    enter = enter_ref[...]
    mixed = local_ref[...] + sum(nt(piece, enter) for piece in split(start_ref[...], 3))
    scale = lax.rsqrt(jnp.mean(mixed * mixed, axis=-1, keepdims=True) + EPSILON)
    gate = jax.nn.silu(gate_ref[...].astype(F32))
    rows = (mixed * scale * gain_ref[...].astype(F32) * gate).astype(BF16)
    for dest in range(4):
        out_ref[dest] = rows


def project_kernel(ids_ref, heads_ref, w0, w1, w2, w3, out_ref):
    part = ids_ref[0]
    for m in (0, 2):
        pair = ((w0, w1), None, (w2, w3))[m]
        total = jnp.zeros((TOK, 256), F32)
        for h in range(4):
            lanes = slice(h * 128, (h + 1) * 128)
            weight = jnp.concatenate([w[:, lanes] for w in pair], axis=1)
            total = total + jnp.dot(heads_ref[h], weight, preferred_element_type=F32)
        out_ref[part ^ m] = total[:, :128].astype(BF16)
        out_ref[part ^ (m + 1)] = total[:, 128:].astype(BF16)


def ranks_of(routing_ref):
    experts = lax.broadcasted_iota(jnp.int32, (TOK, 128), 1)
    hot = [(routing_ref[:, k : k + 1] == experts).astype(F32) for k in range(4)]
    named = hot[0] + hot[1] + hot[2] + hot[3]
    rows = lax.broadcasted_iota(jnp.int32, (TOK, TOK), 0)
    cols = lax.broadcasted_iota(jnp.int32, (TOK, TOK), 1)
    earlier = (rows > cols).astype(F32).astype(BF16)
    ranks = jnp.dot(earlier, named.astype(BF16), preferred_element_type=F32)
    return [jnp.sum(h * ranks, axis=1, keepdims=True).astype(jnp.int32) for h in hot]


def pick_kernel(ids_ref, routing_ref, pick_ref):
    group = ids_ref[1]
    ranks = ranks_of(routing_ref)
    slots = lax.broadcasted_iota(jnp.int32, (TOK, SLOTS), 1)
    picked = jnp.zeros((TOK, SLOTS), F32)
    for k in range(4):
        expert = routing_ref[:, k : k + 1]
        place = ranks[k] * 32 + lax.shift_right_logical(expert, 2)
        place = jnp.where((expert & 3) == group, place, -1)
        picked = picked + (place == slots).astype(F32)
    pick_ref[...] = picked.T.astype(BF16)


def weigh_kernel(routing_ref, score_ref, high_ref, low_ref):
    ranks = ranks_of(routing_ref)
    place = [routing_ref[:, k : k + 1] * MOST + ranks[k] for k in range(4)]
    scores = [score_ref[:, k : k + 1] for k in range(4)]
    total = scores[0] + scores[1] + scores[2] + scores[3]
    slots = lax.broadcasted_iota(jnp.int32, (TOK, 512), 1)
    for j in range(ALL_SLOTS // 512):
        weighted = jnp.zeros((TOK, 512), F32)
        for k in range(4):
            here = (place[k] - j * 512 == slots).astype(F32)
            weighted = weighted + here * (ROUTE_SCALE * scores[k] / total)
        high = weighted.astype(BF16)
        high_ref[:, j * 512 : (j + 1) * 512] = high
        low_ref[:, j * 512 : (j + 1) * 512] = (weighted - high.astype(F32)).astype(BF16)


def mid_kernel(in_ref, residual_ref, out_ref):
    total = residual_ref[...].astype(F32)
    for s in range(4):
        total = total + in_ref[s].astype(F32)
    mid = total.astype(BF16)
    for dest in range(4):
        out_ref[dest] = mid


def dispatch_kernel(pick_ref, mid_ref, out_ref, wide_ref):
    pick = pick_ref[...]
    for q in range(4):
        picked = jnp.dot(pick, mid_ref[q], preferred_element_type=F32)
        for r in range(MOST):
            wide_ref[pl.ds(q * MOST + r, 32, stride=PITCH), :] = picked[r * 32 : (r + 1) * 32]
    for s in range(32):
        out_ref[s * 48 : (s + 1) * 48, :] = wide_ref[s * PITCH : s * PITCH + 48, :].astype(BF16)


def expert_kernel(ready, ids_ref, x0, x1, x2, x3, gain_ref, gate_ref, up_ref, out_ref, wide_ref, rows_ref):
    part = ids_ref[0]
    squares = jnp.zeros((SLOTS, 128), F32)
    for m, x_ref in enumerate((x0, x1, x2, x3)):
        for s in range(32):
            wide_ref[m, s * PITCH : s * PITCH + 48, :] = x_ref[s * 48 : (s + 1) * 48, :].astype(F32)
    for m in range(4):
        for q in range(4):
            slab = q * 4 + (part ^ m)
            tile = jnp.concatenate(
                [wide_ref[m, pl.ds(q * MOST + r, 32, stride=PITCH), :] for r in range(MOST)], axis=0
            )
            squares = squares + tile * tile
            scaled = (tile * gain_ref[pl.ds(slab, 1), :]).astype(BF16)
            rows_ref[:, pl.ds(pl.multiple_of(slab * 128, 128), 128)] = scaled
    scale = lax.rsqrt(jnp.sum(squares, axis=1, keepdims=True) * (1.0 / D) + EPSILON)
    ready()
    gate = jnp.dot(rows_ref[...], gate_ref[...], preferred_element_type=F32) * scale
    up = jnp.dot(rows_ref[...], up_ref[...], preferred_element_type=F32) * scale
    out_ref[...] = (jax.nn.silu(gate) * up).astype(BF16)


def gain_kernel(in_ref, out_ref):
    out_ref[...] = in_ref[...].astype(F32)


def down_kernel(h0, h1, h2, h3, d0, d1, d2, d3, out_ref, wide_ref):
    total = jnp.zeros((SLOTS, 512), F32)
    for h_ref, d_ref in ((h0, d0), (h1, d1), (h2, d2), (h3, d3)):
        total = total + jnp.dot(h_ref[...], d_ref[...], preferred_element_type=F32)
    for q in range(4):
        for r in range(MOST):
            wide_ref[pl.ds(q * MOST + r, 32, stride=PITCH), :] = total[
                r * 32 : (r + 1) * 32, q * 128 : (q + 1) * 128
            ]
    for s in range(32):
        out_ref[s * 48 : (s + 1) * 48, :] = wide_ref[s * PITCH : s * PITCH + 48, :].astype(BF16)


def blocks_kernel(ids_ref, project_ref, shared_ref, *out_refs):
    part = ids_ref[0]
    for m, out_ref in enumerate(out_refs):
        for q in range(4):
            slab = q * 4 + (part ^ m)
            lanes = slice(q * 128, (q + 1) * 128)
            out_ref[0:256, lanes] = project_ref[pl.ds(pl.multiple_of(slab * 256, 256), 256), :]
            columns = pl.ds(pl.multiple_of(slab * 128, 128), 128)
            out_ref[256:320, lanes] = shared_ref[:, columns]


def parts_kernel(ids_ref, down_ref, *out_refs):
    part = ids_ref[0]
    for m, out_ref in enumerate(out_refs):
        for q in range(4):
            columns = pl.ds(pl.multiple_of((q * 4 + (part ^ m)) * 128, 128), 128)
            out_ref[:, q * 128 : (q + 1) * 128] = down_ref[:, columns]


def shared_in_kernel(ids_ref, mid_ref, w0, w1, w2, w3, gain_ref, out_ref, weight_ref):
    part = ids_ref[0]
    for m, w_ref in enumerate((w0, w1, w2, w3)):
        at = (part ^ m) * 32
        weight_ref[pl.ds(pl.multiple_of(at, 32), 32), :] = w_ref[256:288, :]
        weight_ref[pl.ds(pl.multiple_of(at + 128, 32), 32), :] = w_ref[288:320, :]
    squares = jnp.zeros((TOK, 128), F32)
    pre = jnp.zeros((TOK, 256), F32)
    for q in range(4):
        tile = mid_ref[q].astype(F32)
        squares = squares + tile * tile
        scaled = (tile * gain_ref[pl.ds(q * 4 + part, 1), :]).astype(BF16)
        pre = pre + nt(scaled, weight_ref[:, q * 128 : (q + 1) * 128])
    ssq = jnp.sum(squares, axis=1, keepdims=True)
    high = ssq.astype(BF16).astype(F32)
    lane = lax.broadcasted_iota(jnp.int32, (TOK, 128), 1)
    tail = jnp.where(lane == 0, high, jnp.where(lane == 1, ssq - high, 0.0)).astype(BF16)
    out_ref[:, 0:256] = pre.astype(BF16)
    out_ref[:, 256:384] = tail


def shared_hidden_kernel(r0, r1, r2, r3, out_ref):
    total = sum(r[...].astype(F32) for r in (r0, r1, r2, r3))
    ssq = jnp.sum(total[:, 256:384], axis=1, keepdims=True)
    scale = lax.rsqrt(ssq * (1.0 / D) + EPSILON)
    hidden = jax.nn.silu(total[:, 0:128] * scale) * (total[:, 128:256] * scale)
    out_ref[...] = hidden.astype(BF16)


def ahead_kernel(ids_ref, h0, h1, h2, h3, down_ref, mid_ref, out_ref):
    group = ids_ref[1]
    total = mid_ref[0].astype(F32)
    for d, h in enumerate((h0, h1, h2, h3)):
        at = pl.multiple_of(((group - d) & 3) * 128, 128)
        total = total + jnp.dot(
            h[...], down_ref[pl.ds(at, 128), :], preferred_element_type=F32
        )
    out_ref[...] = total


def final_kernel(back_ref, high_ref, low_ref, ahead_ref, out_ref):
    back = back_ref[...]
    total = ahead_ref[...] + jnp.dot(high_ref[...], back, preferred_element_type=F32)
    total = total + jnp.dot(low_ref[...], back, preferred_element_type=F32)
    out_ref[...] = total.astype(BF16)


def exchange(value, axes):
    return lax.all_to_all(value, axes, split_axis=0, concat_axis=0, tiled=True)


def moved(value, axes, target):
    count = lax.axis_size(axes)
    return lax.ppermute(value, axes, [(i, target(i) % count) for i in range(count)])


def shifted(values, axes):
    return [moved(v, axes, lambda i, d=d: i + d) for d, v in enumerate(values, 1)]


def swapped(value, axis):
    return moved(value, axis, lambda i: i ^ 1)


def grouped(values):
    return [moved(v, GROUP, lambda i, m=m: i ^ m) for m, v in enumerate(values, 1)]


def body(
    queries,
    key_matrix,
    value_matrix,
    output_gate_preactivation,
    decay_preactivation,
    extra_log_decay,
    head_norm_gain,
    output_projection,
    residual,
    feedforward_gain,
    routing,
    router_score,
    expert_gate_weight,
    expert_up_weight,
    expert_down_weight,
    shared_expert_gate,
    shared_expert_up,
    shared_expert_down,
):
    ids = jnp.stack([lax.axis_index(a) for a in (GROUP, "yg")]).astype(jnp.int32)
    gain = call(gain_kernel, ((16, 128), F32), feedforward_gain.reshape(16, 128))
    head_gain = head_norm_gain.reshape(1, DV)
    extra = extra_log_decay.reshape(2, 128)
    whole = (0, TOK)

    payload = call(
        state_kernel, ((32, 16, DK), BF16),
        key_matrix, value_matrix, decay_preactivation, extra, fetch=(whole, whole, whole, (0, 2)), limit=60,
    )
    states = exchange(payload, SP)
    local, start = call(
        local_kernel, [((TOK, DV), F32), ((TOK, DK), F32)],
        queries, key_matrix, value_matrix, decay_preactivation, extra,
        fetch=(whole, whole, whole, whole, (0, 2)), limit=60,
    )
    pick = call(pick_kernel, ((SLOTS, TOK), BF16), ids, routing, smem=1)
    high, low = call(
        weigh_kernel, [((TOK, ALL_SLOTS), BF16), ((TOK, ALL_SLOTS), BF16)], routing, router_score
    )
    shared_in = jnp.concatenate([shared_expert_gate.T, shared_expert_up.T], axis=0)
    own_block, *far_blocks = call(
        blocks_kernel, [((320, 512), BF16)] * 4, ids, output_projection, shared_in, smem=1,
    )
    blocks = [own_block] + grouped(far_blocks)
    own_part, *far_parts = call(
        parts_kernel, [((256, 512), BF16)] * 4, ids, expert_down_weight, smem=1,
    )
    parts = [own_part] + grouped(far_parts)

    entering = exchange(call(scan_kernel, ((32, 8, DK), BF16), states), SP)
    head_rows = call(
        head_kernel, ((4, TOK, DV), BF16),
        entering.reshape(DV, DK), head_gain, local, start, output_gate_preactivation,
        fetch=(whole,) * 3,
    )
    partial = call(
        project_kernel, ((4, TOK, 128), BF16),
        ids, exchange(head_rows, "yg"), *blocks, smem=1, fetch=(whole,) * 4,
    )
    mid = call(mid_kernel, ((4, TOK, 128), BF16), exchange(partial, GROUP), residual)
    mid_part = exchange(mid, "yg")
    outgoing = call(
        dispatch_kernel, ((ALL_SLOTS, 128), BF16), pick, mid_part,
        scratch=[pltpu.VMEM((32 * PITCH, 128), F32)],
    )
    own = exchange(outgoing.reshape(32, 48, 128), SP).reshape(ALL_SLOTS, 128)

    across = swapped(own, "yn")
    beside = swapped(own, "c")
    far = swapped(across, "c")
    pre = call(
        shared_in_kernel, ((TOK, 384), BF16), ids, mid_part, *blocks, gain, smem=1,
        scratch=[pltpu.VMEM((256, 512), BF16)],
    )
    pre = [pre] + grouped([pre] * 3)
    routed = call(
        expert_kernel, ((SLOTS, 256), BF16),
        ids, own, beside, across, far, gain, expert_gate_weight, expert_up_weight,
        smem=1, fetch=((0, D), (0, D)), late=True,
        scratch=[pltpu.VMEM((4, 32 * PITCH, 128), F32), pltpu.VMEM((SLOTS, D), BF16)],
    )
    routed_across = swapped(routed, "yn")
    routed_beside = swapped(routed, "c")
    routed_far = swapped(routed_across, "c")
    expert_out = call(
        down_kernel, ((ALL_SLOTS, 128), BF16),
        routed, routed_beside, routed_across, routed_far, *parts,
        scratch=[pltpu.VMEM((32 * PITCH, 128), F32)],
    )
    back = exchange(expert_out.reshape(128, 3, 4, 128), SPG).reshape(ALL_SLOTS, 128)
    hidden = call(shared_hidden_kernel, ((TOK, 128), BF16), *pre)
    hidden = [hidden] + shifted([hidden] * 3, "yg")
    ahead = call(
        ahead_kernel, ((TOK, 128), F32), ids, *hidden, shared_expert_down, mid, smem=1,
    )
    return call(final_kernel, ((TOK, 128), BF16), back, high, low, ahead)


def solution(mesh):
    finer = Mesh(mesh.devices.reshape(8, 4, 4, 2, 2), ("z", "x", "yg", "yn", "c"))
    in_specs = (
        P(SP, TP),
        P(SP, TP),
        P(SP, TP),
        P(SP, TP),
        P(SP, TP),
        P(SP, TP),
        P(),
        P(None, TP),
        P(SP, TP),
        P(),
        P(SP, None),
        P(SP, None),
        P(None, SP + TP),
        P(None, SP + TP),
        P(SP + TP, None),
        P(None, TP),
        P(None, TP),
        P(None, TP),
    )
    return jax.shard_map(body, mesh=finer, in_specs=in_specs, out_specs=P(SP, TP), check_vma=False)
```

```python
import jax
import jax.numpy as jnp
from jax import lax
from jax.experimental import pallas as pl
from jax.experimental.pallas import tpu as pltpu
from jax.sharding import Mesh
from jax.sharding import PartitionSpec as P

DK = 128
DV = 256
BLOCK = 64
TOK = 256
MOST = 12
SLOTS = 384
ALL_SLOTS = 1536
D = 2048
SP = ("z", "x")
GSP = ("yg", "z", "x")
TP = ("yg", "yn", "c")
GROUP = ("yn", "c")
F32 = jnp.float32
BF16 = jnp.bfloat16
HIGHEST = lax.Precision.HIGHEST
EPSILON = 1e-06
ROUTE_SCALE = 2.5
GATE_TEMPER = 16.0
VMEM = pl.BlockSpec(memory_space=pltpu.VMEM)
SMEM = pl.BlockSpec(memory_space=pltpu.SMEM)


def call(kernel, outs, *args, scratch=(), smem=0, fetch=(), late=False, limit=24):
    single = not isinstance(outs, list)
    shapes = [jax.ShapeDtypeStruct(s, t) for s, t in ([outs] if single else outs)]
    n_in, n_out, n_scratch, n_fetch = len(args), len(shapes), len(scratch), len(fetch)
    kept = n_in - n_fetch
    buffers = []
    for arg, rows in zip(args[kept:], fetch, strict=True):
        buffers.append(pltpu.VMEM((rows[1], *arg.shape[1:]), arg.dtype))

    def fetching(*refs):
        sources, results = refs[kept:n_in], refs[n_in : n_in + n_out]
        own = refs[n_in + n_out : n_in + n_out + n_scratch]
        held, sems = refs[n_in + n_out + n_scratch : -1], refs[-1]
        copies = [
            pltpu.make_async_copy(src.at[pl.ds(rows[0], rows[1])], dst, sems.at[i])
            for i, (src, dst, rows) in enumerate(zip(sources, held, fetch, strict=True))
        ]
        for copy in copies:
            copy.start()

        def ready():
            for copy in copies:
                copy.wait()

        if late:
            kernel(ready, *refs[:kept], *held, *results, *own)
        else:
            ready()
            kernel(*refs[:kept], *held, *results, *own)

    extra = buffers + [pltpu.SemaphoreType.DMA((n_fetch,))] if fetch else []
    any_spec = pl.BlockSpec(memory_space=pl.ANY)
    got = pl.pallas_call(
        fetching if fetch else kernel,
        out_shape=shapes,
        in_specs=[SMEM] * smem + [VMEM] * (kept - smem) + [any_spec] * n_fetch,
        out_specs=[VMEM] * n_out,
        scratch_shapes=list(scratch) + extra,
        compiler_params=pltpu.CompilerParams(vmem_limit_bytes=limit * 2**20),
        cost_estimate=pl.CostEstimate(
            flops=1000000, bytes_accessed=1000000, transcendentals=0
        ),
    )(*args)
    return got[0] if single else got


def nt(a, b, **kw):
    return lax.dot_general(
        a, b, (((1,), (1,)), ((), ())), preferred_element_type=F32, **kw
    )


def split(value, count):
    pieces = []
    for _ in range(count):
        piece = value.astype(BF16)
        pieces.append(piece)
        value = value - piece.astype(F32)
    return pieces


def dot(a, b):
    return jnp.dot(a, b, preferred_element_type=F32)


def decays(decay_ref, extra_ref):
    raw = decay_ref[...].astype(F32)
    logs = jax.nn.log_sigmoid(raw) / GATE_TEMPER
    rows = lax.broadcasted_iota(jnp.int32, (BLOCK, BLOCK), 0)
    cols = lax.broadcasted_iota(jnp.int32, (BLOCK, BLOCK), 1)
    lower = (rows >= cols).astype(F32).astype(BF16)
    wide_rows = lax.broadcasted_iota(jnp.int32, (BLOCK, 128), 0)
    wide_cols = lax.broadcasted_iota(jnp.int32, (BLOCK, 128), 1)
    ones = jnp.ones((128, DK), BF16)
    inside = []
    for b in range(TOK // BLOCK):
        at = wide_cols - (b % 2) * BLOCK
        extra = jnp.where((at >= 0) & (at <= wide_rows), extra_ref[b // 2 : b // 2 + 1, :], 0.0)
        total = sum(dot(lower, piece) for piece in split(logs[b * BLOCK : (b + 1) * BLOCK], 3))
        inside.append(total + sum(dot(piece, ones) for piece in split(extra, 3)))
    return inside


def block_states(inside, key_ref, value_ref):
    state = jnp.zeros((DV, DK), F32)
    states = []
    total = jnp.zeros((1, DK), F32)
    for b, cum in enumerate(inside):
        states.append(state)
        rows = pl.ds(b * BLOCK, BLOCK)
        end = cum[BLOCK - 1 : BLOCK]
        key_end = key_ref[rows, :].astype(F32) * jnp.exp(end - cum)
        value = value_ref[rows, :].astype(F32)
        fresh = jnp.dot(value.T, key_end, precision=HIGHEST, preferred_element_type=F32)
        state = jnp.exp(end) * state + fresh
        total = total + end
    return states, state, total


def state_kernel(key_ref, value_ref, decay_ref, extra_ref, out_ref):
    inside = decays(decay_ref, extra_ref)
    later = jnp.zeros((1, DK), F32)
    scaled = []
    for cum in reversed(inside):
        end = cum[BLOCK - 1 : BLOCK]
        scaled.insert(0, jnp.exp(end - cum + later))
        later = later + end
    key_end = key_ref[...].astype(F32) * jnp.concatenate(scaled, axis=0)
    value_t = value_ref[...].astype(F32).T.astype(BF16)
    state = sum(dot(value_t, piece) for piece in split(key_end, 3))
    out_ref[:, 0:8, :] = state.reshape(32, 8, DK).astype(BF16)
    decay = jnp.exp(later)
    high = decay.astype(BF16).astype(F32)
    row = lax.broadcasted_iota(jnp.int32, (8, DK), 0)
    tail = jnp.where(row == 0, high, jnp.where(row == 1, decay - high, 0.0))
    out_ref[:, 8:16, :] = jnp.broadcast_to(tail[None], (32, 8, DK)).astype(BF16)


def scan_kernel(in_ref, out_ref):
    state = jnp.zeros((8, DK), F32)
    for s in range(32):
        out_ref[s] = state.astype(BF16)
        block = in_ref[s].astype(F32)
        decay = block[8:9] + block[9:10]
        state = decay * state + block[0:8]


def local_kernel(query_ref, key_ref, value_ref, decay_ref, extra_ref, local_ref, start_ref):
    inside = decays(decay_ref, extra_ref)
    states, _, _ = block_states(inside, key_ref, value_ref)
    rows_at = lax.broadcasted_iota(jnp.int32, (BLOCK, BLOCK), 0)
    cols_at = lax.broadcasted_iota(jnp.int32, (BLOCK, BLOCK), 1)
    before = jnp.zeros((1, DK), F32)
    for b, cum in enumerate(inside):
        rows = pl.ds(b * BLOCK, BLOCK)
        query = query_ref[rows, :].astype(F32) * DK ** (-0.5)
        key = key_ref[rows, :].astype(F32)
        value = value_ref[rows, :].astype(F32)
        query_decay = query * jnp.exp(cum)
        scores = nt(query_decay, key * jnp.exp(-cum), precision=HIGHEST)
        scores = jnp.where(rows_at >= cols_at, scores, 0.0)
        mixed = jnp.dot(scores, value, precision=HIGHEST, preferred_element_type=F32)
        if b > 0:
            mixed = mixed + nt(query_decay, states[b], precision=HIGHEST)
        local_ref[rows, :] = mixed
        start_ref[rows, :] = query * jnp.exp(cum + before)
        before = before + cum[BLOCK - 1 : BLOCK]


def head_kernel(enter_ref, gain_ref, local_ref, start_ref, gate_ref, out_ref):
    enter = enter_ref[...]
    mixed = local_ref[...] + sum(nt(piece, enter) for piece in split(start_ref[...], 3))
    scale = lax.rsqrt(jnp.mean(mixed * mixed, axis=-1, keepdims=True) + EPSILON)
    gate = jax.nn.silu(gate_ref[...].astype(F32))
    rows = (mixed * scale * gain_ref[...].astype(F32) * gate).astype(BF16)
    for dest in range(4):
        out_ref[dest] = rows


def project_kernel(ids_ref, heads_ref, w0, w1, w2, w3, out_ref):
    part = ids_ref[0]
    for m in (0, 2):
        pair = ((w0, w1), None, (w2, w3))[m]
        total = jnp.zeros((TOK, 256), F32)
        for h in range(4):
            lanes = slice(h * 128, (h + 1) * 128)
            weight = jnp.concatenate([w[:, lanes] for w in pair], axis=1)
            total = total + jnp.dot(heads_ref[h], weight, preferred_element_type=F32)
        out_ref[part ^ m] = total[:, :128].astype(BF16)
        out_ref[part ^ (m + 1)] = total[:, 128:].astype(BF16)


def places(routing_ref):
    experts = lax.broadcasted_iota(jnp.int32, (TOK, 128), 1)
    hot = [(routing_ref[:, k : k + 1] == experts).astype(F32) for k in range(4)]
    named = hot[0] + hot[1] + hot[2] + hot[3]
    rows = lax.broadcasted_iota(jnp.int32, (TOK, TOK), 0)
    cols = lax.broadcasted_iota(jnp.int32, (TOK, TOK), 1)
    earlier = (rows > cols).astype(BF16)
    ranks = jnp.dot(earlier, named.astype(BF16), preferred_element_type=F32)
    slots = []
    for k in range(4):
        expert = routing_ref[:, k : k + 1]
        place = (expert & 3) * 32 + lax.shift_right_logical(expert, 2)
        rank = jnp.sum(hot[k] * ranks, axis=1, keepdims=True).astype(jnp.int32)
        slots.append(place * MOST + rank)
    return slots


def pick_kernel(routing_ref, pick_ref):
    place = places(routing_ref)
    slots = lax.broadcasted_iota(jnp.int32, (TOK, 512), 1)
    for j in range(ALL_SLOTS // 512):
        picked = jnp.zeros((TOK, 512), F32)
        for k in range(4):
            picked = picked + (place[k] - j * 512 == slots).astype(F32)
        pick_ref[j * 512 : (j + 1) * 512, :] = picked.T.astype(BF16)


def weigh_kernel(routing_ref, score_ref, high_ref, low_ref):
    place = places(routing_ref)
    scores = [score_ref[:, k : k + 1] for k in range(4)]
    total = scores[0] + scores[1] + scores[2] + scores[3]
    slots = lax.broadcasted_iota(jnp.int32, (TOK, 512), 1)
    for j in range(ALL_SLOTS // 512):
        weighted = jnp.zeros((TOK, 512), F32)
        for k in range(4):
            here = (place[k] - j * 512 == slots).astype(F32)
            weighted = weighted + here * (ROUTE_SCALE * scores[k] / total)
        high = weighted.astype(BF16)
        high_ref[:, j * 512 : (j + 1) * 512] = high
        low_ref[:, j * 512 : (j + 1) * 512] = (weighted - high.astype(F32)).astype(BF16)


def dispatch_kernel(pick_ref, in_ref, residual_ref, out_ref, mid_ref):
    total = residual_ref[...].astype(F32)
    for s in range(4):
        total = total + in_ref[s].astype(F32)
    mid = total.astype(BF16)
    mid_ref[...] = mid
    for j in range(4):
        rows = pl.ds(j * SLOTS, SLOTS)
        picked = jnp.dot(pick_ref[rows, :], mid, preferred_element_type=F32)
        out_ref[rows, :] = picked.astype(BF16)


def expert_kernel(ready, ids_ref, x0, x1, x2, x3, gain_ref, gate_ref, up_ref, out_ref, rows_ref):
    part = ids_ref[0]
    squares = jnp.zeros((SLOTS, 128), F32)
    for m, x_ref in enumerate((x0, x1, x2, x3)):
        for q in range(4):
            slab = q * 4 + (part ^ m)
            tile = x_ref[q * SLOTS : (q + 1) * SLOTS, :].astype(F32)
            squares = squares + tile * tile
            scaled = (tile * gain_ref[pl.ds(slab, 1), :]).astype(BF16)
            rows_ref[:, pl.ds(pl.multiple_of(slab * 128, 128), 128)] = scaled
    scale = lax.rsqrt(jnp.sum(squares, axis=1, keepdims=True) * (1.0 / D) + EPSILON)
    ready()
    gate = jnp.dot(rows_ref[...], gate_ref[...], preferred_element_type=F32) * scale
    up = jnp.dot(rows_ref[...], up_ref[...], preferred_element_type=F32) * scale
    out_ref[...] = (jax.nn.silu(gate) * up).astype(BF16)


def gain_kernel(in_ref, out_ref):
    out_ref[...] = in_ref[...].astype(F32)


def down_kernel(h0, h1, h2, h3, d0, d1, d2, d3, out_ref):
    total = jnp.zeros((SLOTS, 512), F32)
    for h_ref, d_ref in ((h0, d0), (h1, d1), (h2, d2), (h3, d3)):
        total = total + jnp.dot(h_ref[...], d_ref[256:512, :], preferred_element_type=F32)
    for q in range(4):
        out_ref[q * SLOTS : (q + 1) * SLOTS, :] = total[:, q * 128 : (q + 1) * 128].astype(BF16)


def parts_kernel(ids_ref, project_ref, down_ref, shared_ref, *out_refs):
    part = ids_ref[0]
    for m, out_ref in enumerate(out_refs):
        for q in range(4):
            slab = q * 4 + (part ^ m)
            lanes = slice(q * 128, (q + 1) * 128)
            out_ref[0:256, lanes] = project_ref[pl.ds(pl.multiple_of(slab * 256, 256), 256), :]
            columns = pl.ds(pl.multiple_of(slab * 128, 128), 128)
            out_ref[256:512, lanes] = down_ref[:, columns]
            out_ref[512:576, lanes] = shared_ref[:, columns]


def shared_in_kernel(ids_ref, m0, m1, m2, m3, w0, w1, w2, w3, gain_ref, out_ref, weight_ref, mid_ref):
    part, group = ids_ref[0], ids_ref[1]
    for m, w_ref in enumerate((w0, w1, w2, w3)):
        at = (part ^ m) * 32
        weight_ref[pl.ds(pl.multiple_of(at, 32), 32), :] = w_ref[512:544, :]
        weight_ref[pl.ds(pl.multiple_of(at + 128, 32), 32), :] = w_ref[544:576, :]
    for d, m_ref in enumerate((m0, m1, m2, m3)):
        mid_ref[(group - d) & 3] = m_ref[...]
    squares = jnp.zeros((TOK, 128), F32)
    pre = jnp.zeros((TOK, 256), F32)
    for q in range(4):
        tile = mid_ref[q].astype(F32)
        squares = squares + tile * tile
        scaled = (tile * gain_ref[pl.ds(q * 4 + part, 1), :]).astype(BF16)
        pre = pre + nt(scaled, weight_ref[:, q * 128 : (q + 1) * 128])
    ssq = jnp.sum(squares, axis=1, keepdims=True)
    high = ssq.astype(BF16).astype(F32)
    lane = lax.broadcasted_iota(jnp.int32, (TOK, 128), 1)
    tail = jnp.where(lane == 0, high, jnp.where(lane == 1, ssq - high, 0.0)).astype(BF16)
    out_ref[:, 0:256] = pre.astype(BF16)
    out_ref[:, 256:384] = tail


def shared_hidden_kernel(r0, r1, r2, r3, out_ref):
    total = sum(r[...].astype(F32) for r in (r0, r1, r2, r3))
    ssq = jnp.sum(total[:, 256:384], axis=1, keepdims=True)
    scale = lax.rsqrt(ssq * (1.0 / D) + EPSILON)
    hidden = jax.nn.silu(total[:, 0:128] * scale) * (total[:, 128:256] * scale)
    out_ref[...] = hidden.astype(BF16)


def ahead_kernel(ids_ref, h0, h1, h2, h3, down_ref, mid_ref, out_ref):
    group = ids_ref[1]
    total = mid_ref[...].astype(F32)
    for d, h in enumerate((h0, h1, h2, h3)):
        at = pl.multiple_of(((group - d) & 3) * 128, 128)
        total = total + jnp.dot(
            h[...], down_ref[pl.ds(at, 128), :], preferred_element_type=F32
        )
    out_ref[...] = total


def final_kernel(back_ref, high_ref, low_ref, ahead_ref, out_ref):
    back = back_ref[...]
    total = ahead_ref[...] + jnp.dot(high_ref[...], back, preferred_element_type=F32)
    total = total + jnp.dot(low_ref[...], back, preferred_element_type=F32)
    out_ref[...] = total.astype(BF16)


def exchange(value, axes):
    return lax.all_to_all(value, axes, split_axis=0, concat_axis=0, tiled=True)


def moved(value, axes, target):
    count = lax.axis_size(axes)
    return lax.ppermute(value, axes, [(i, target(i) % count) for i in range(count)])


def shifted(values, axes):
    return [moved(v, axes, lambda i, d=d: i + d) for d, v in enumerate(values, 1)]


def swapped(value, axis):
    return moved(value, axis, lambda i: i ^ 1)


def grouped(values):
    return [moved(v, GROUP, lambda i, m=m: i ^ m) for m, v in enumerate(values, 1)]


def body(
    queries,
    key_matrix,
    value_matrix,
    output_gate_preactivation,
    decay_preactivation,
    extra_log_decay,
    head_norm_gain,
    output_projection,
    residual,
    feedforward_gain,
    routing,
    router_score,
    expert_gate_weight,
    expert_up_weight,
    expert_down_weight,
    shared_expert_gate,
    shared_expert_up,
    shared_expert_down,
):
    ids = jnp.stack([lax.axis_index(a) for a in (GROUP, "yg")]).astype(jnp.int32)
    gain = call(gain_kernel, ((16, 128), F32), feedforward_gain.reshape(16, 128))
    head_gain = head_norm_gain.reshape(1, DV)
    extra = extra_log_decay.reshape(2, 128)
    whole = (0, TOK)

    payload = call(
        state_kernel, ((32, 16, DK), BF16),
        key_matrix, value_matrix, decay_preactivation, extra, fetch=(whole, whole, whole, (0, 2)), limit=60,
    )
    states = exchange(payload, SP)
    local, start = call(
        local_kernel, [((TOK, DV), F32), ((TOK, DK), F32)],
        queries, key_matrix, value_matrix, decay_preactivation, extra,
        fetch=(whole, whole, whole, whole, (0, 2)), limit=60,
    )
    pick = call(pick_kernel, ((ALL_SLOTS, TOK), BF16), routing)
    high, low = call(
        weigh_kernel, [((TOK, ALL_SLOTS), BF16), ((TOK, ALL_SLOTS), BF16)], routing, router_score
    )
    shared_in = jnp.concatenate([shared_expert_gate.T, shared_expert_up.T], axis=0)
    own_part, *far_parts = call(
        parts_kernel, [((576, 512), BF16)] * 4,
        ids, output_projection, expert_down_weight, shared_in, smem=1,
    )
    parts = [own_part] + grouped(far_parts)

    entering = exchange(call(scan_kernel, ((32, 8, DK), BF16), states), SP)
    head_rows = call(
        head_kernel, ((4, TOK, DV), BF16),
        entering.reshape(DV, DK), head_gain, local, start, output_gate_preactivation,
        fetch=(whole,) * 3, limit=60,
    )
    partial = call(
        project_kernel, ((4, TOK, 128), BF16),
        ids, exchange(head_rows, "yg"), *parts, smem=1, fetch=(whole,) * 4,
    )
    outgoing, mid = call(
        dispatch_kernel, [((ALL_SLOTS, 128), BF16), ((TOK, 128), BF16)],
        pick, exchange(partial, GROUP), residual,
    )
    own = exchange(outgoing.reshape(128, 3, 4, 128), GSP).reshape(ALL_SLOTS, 128)
    mids = [mid] + shifted([mid] * 3, "yg")

    across = swapped(own, "yn")
    beside = swapped(own, "c")
    far = swapped(across, "c")
    pre = call(
        shared_in_kernel, ((TOK, 384), BF16), ids, *mids, *parts, gain, smem=1,
        scratch=[pltpu.VMEM((256, 512), BF16), pltpu.VMEM((4, TOK, 128), BF16)],
    )
    pre = [pre] + grouped([pre] * 3)
    routed = call(
        expert_kernel, ((SLOTS, 256), BF16),
        ids, own, beside, across, far, gain, expert_gate_weight, expert_up_weight,
        smem=1, fetch=((0, D), (0, D)), late=True,
        scratch=[pltpu.VMEM((SLOTS, D), BF16)],
    )
    routed_across = swapped(routed, "yn")
    routed_beside = swapped(routed, "c")
    routed_far = swapped(routed_across, "c")
    expert_out = call(
        down_kernel, ((ALL_SLOTS, 128), BF16),
        routed, routed_beside, routed_across, routed_far, *parts,
    )
    back = exchange(expert_out.reshape(128, 3, 4, 128), GSP).reshape(ALL_SLOTS, 128)
    hidden = call(shared_hidden_kernel, ((TOK, 128), BF16), *pre)
    hidden = [hidden] + shifted([hidden] * 3, "yg")
    ahead = call(
        ahead_kernel, ((TOK, 128), F32), ids, *hidden, shared_expert_down, mid, smem=1,
    )
    return call(final_kernel, ((TOK, 128), BF16), back, high, low, ahead)


def solution(mesh):
    finer = Mesh(mesh.devices.reshape(8, 4, 4, 2, 2), ("z", "x", "yg", "yn", "c"))
    in_specs = (
        P(SP, TP),
        P(SP, TP),
        P(SP, TP),
        P(SP, TP),
        P(SP, TP),
        P(SP, TP),
        P(),
        P(None, TP),
        P(SP, TP),
        P(),
        P(SP, None),
        P(SP, None),
        P(None, SP + TP),
        P(None, SP + TP),
        P(SP + TP, None),
        P(None, TP),
        P(None, TP),
        P(None, TP),
    )
    return jax.shard_map(body, mesh=finer, in_specs=in_specs, out_specs=P(SP, TP), check_vma=False)
```
